32 devices in a mesh: ep: 8 (over z, x), tp: 4 (over y, core).
Axes of the slice: x: 2, y: 2, z: 4, core: 2. Of those that a mesh axis runs over, the one named last changes fastest.
Arguments:
- pool_in: bfloat16 [8192, 1024], P(('ep', 'tp')), may hold values from -6 to 6
- w_pool: bfloat16 [8, 128, 128], replicated, may hold values from -0.5 to 0.5
- pool_scale: float32 [1024], replicated, may hold values from 0.1 to 1.9
- w_out: bfloat16 [1024, 2048], replicated, may hold values from -0.1875 to 0.1875
- expert_in: bfloat16 [4096, 2048], P('ep'), may hold values from -6 to 6
- ffn_gain: float32 [2048], replicated, may hold values from 0.1 to 1.9
- routes: int32 [4096, 2], P('ep'), may hold values from 0 to 7, all different within a row; in each aligned block of 128 rows (0 to 127, 128 to 255, ...) at most 48 rows name the same one
- route_weight: float32 [4096, 2], P('ep'), may hold values from 0.25 to 1
- w_gate: bfloat16 [8, 2048, 1024], P('ep', None, 'tp'), may hold values from -0.125 to 0.125
- w_up: bfloat16 [8, 2048, 1024], P('ep', None, 'tp'), may hold values from -0.125 to 0.125
- w_down: bfloat16 [8, 1024, 2048], P('ep', 'tp'), may hold values from -0.1875 to 0.1875
Outputs:
- mixer_out: bfloat16 [8192, 2048], P(('ep', 'tp'))
- expert_out: bfloat16 [4096, 2048], P(('ep', 'tp'))
The draws below stay inside these ranges and needn't reach their ends.
Inputs may be any that keep to these rules, and one draw needn't show every extreme that they name: `routes`: each row names 2 different experts. In each aligned block of 128 rows no expert is named by more than 48 rows, and in some block some expert is named by exactly 48 rows.
All inputs are finite; a program needn't handle non-finite values.
Results may differ from the reference program's by a relative error of at most 0.012.
Values may be sent and summed in bfloat16 or wider, within the bound.
A program may use at most 128 MiB of HBM per device.

```python
import math
import jax
import jax.numpy as jnp
import numpy as np
from jax import lax

D = 2048
GDIM = 128
GROUPS = 8
PW = 1024
WMAX = 16
FF_E = 1024
EXPERTS = 8
K = 2
TB_DEV = 128
CAP = 48
TOKENS_A = 8192
TOKENS_B = 4096
N_EP = 8
N_TP = 4


def steps_of(stream_key, shape, cuts, smallest, largest):
    def one(axis_at, shards_of):
        steps = jax.random.uniform(jax.random.fold_in(jax.random.fold_in(stream_key, 6), axis_at), (shards_of,), jnp.float32, smallest / len(cuts), largest / len(cuts))
        return jnp.repeat(jnp.exp(steps), shape[axis_at] // shards_of).reshape((-1,) + (1,) * (len(shape) - axis_at - 1))

    factor_of = one(*cuts[0])
    for cut in cuts[1:]:
        factor_of = factor_of * one(*cut)
    return factor_of


def routed_block(stream_key, own, number, rows, count, top, limit, skew):
    sequence = jax.random.permutation(stream_key, count)
    crowded, ordinary = load_shares(count, rows * top, limit, skew, True), load_shares(count, rows * top, limit, skew, False)
    places = jnp.arange(count)

    def named(sizes, rotation):
        used = int((sizes > 0).sum())
        fixed = max(1, used // 4)
        passed = fixed + (places - fixed + rotation * (used - fixed)) % max(1, count - fixed)
        return jnp.zeros((count,), jnp.int32).at[sequence[jnp.where(places < fixed, places, passed)]].set(jnp.asarray(sizes, jnp.int32))

    sizes = jnp.where(number % 4 == 0, named(crowded, number // 4), named(ordinary, number - number // 4 - 1))
    mixed = jax.random.permutation(jax.random.fold_in(own, 3), count)
    donor, receiver = mixed[0:count // 2 * 2:2], mixed[1:count // 2 * 2:2]
    room = jnp.minimum(sizes[donor] - 1, limit - sizes[receiver]) // 2
    room = jnp.where((donor == sequence[0]) | (receiver == sequence[0]) | (sizes[receiver] == 0), 0, jnp.maximum(room, 0))
    passed = jax.random.randint(jax.random.fold_in(own, 4), (count // 2,), 0, 1 << 20) % (room + 1)
    sizes = sizes.at[donor].add(-passed).at[receiver].add(passed)
    labels = jnp.searchsorted(jnp.cumsum(sizes), jnp.arange(rows * top), side="right").astype(jnp.int32)
    listing = labels.reshape(top, rows).T
    listing = listing[jax.random.permutation(jax.random.fold_in(own, 1), rows)]
    rotation = jax.random.randint(jax.random.fold_in(own, 2), (rows, 1), 0, top)
    return jnp.take_along_axis(listing, (jnp.arange(top)[None, :] + rotation) % top, axis=1)


def load_shares(count, total, reach, skew, full):
    weights = [(1 << 20) // math.isqrt(standing ** skew) + 1 for standing in range(1, count + 1)]
    largest = reach if full else min(reach, max(-(-total // count), total * weights[0] // sum(weights)))
    least = 1 if total - largest >= count - 1 else 0
    counts, surplus = [largest] + [least] * (count - 1), total - largest - least * (count - 1)
    while surplus > 0:
        candidates = [i for i in range(1, count) if counts[i] < largest] or [i for i in range(1, count) if counts[i] < reach]
        mass, budget = sum([weights[i] for i in candidates]), surplus
        for i in candidates:
            more = min(reach - counts[i], max(1, budget * weights[i] // mass), surplus)
            counts[i] = counts[i] + more
            surplus = surplus - more
    return np.array(counts)


def scatter_about(stream_key, dims, scale, most, split=(), kind=jnp.bfloat16):
    array = scale * jax.random.normal(stream_key, dims, jnp.float32)
    if split:
        array = array * steps_of(stream_key, dims, split, -0.22, 0.18)
    return jnp.clip(array, -most, most).astype(kind)


def setup_inputs(seed: int = 0) -> dict:
    key_of = jax.random.split(jax.random.key(seed), 12)
    pool_in = scatter_about(key_of[0], (TOKENS_A, PW), 1.0, 6.0, ((0, 32),))
    w_pool = scatter_about(key_of[1], (GROUPS, GDIM, GDIM), GDIM ** -0.5, 0.5)
    pool_scale = jnp.clip(1.0 + 0.18 * jax.random.normal(key_of[2], (PW,), jnp.float32), 0.1, 1.9)
    w_out = scatter_about(key_of[3], (PW, D), PW ** -0.5, 0.1875)
    expert_in = scatter_about(key_of[4], (TOKENS_B, D), 1.0, 6.0, ((0, 8),))
    ffn_gain = jnp.clip(1.0 + 0.18 * jax.random.normal(key_of[5], (D,), jnp.float32), 0.1, 1.9)
    routes_keys = jax.random.split(jax.random.fold_in(key_of[6], 1), TOKENS_B // TB_DEV)
    routes_turns = jax.random.permutation(jax.random.fold_in(key_of[6], 3), TOKENS_B // TB_DEV)
    routes = jax.vmap(lambda own, number: routed_block(jax.random.fold_in(key_of[6], 2), own, number, TB_DEV, EXPERTS, K, CAP, 1))(routes_keys, routes_turns).reshape((TOKENS_B, K))
    route_weight = jnp.clip(0.25 + 0.75 * jax.random.uniform(key_of[7], (TOKENS_B, K), jnp.float32) ** steps_of(key_of[7], (TOKENS_B, K), ((0, 8),), -0.2, 0.2), 0.25, 1.0)
    w_gate = scatter_about(key_of[8], (EXPERTS, D, FF_E), D ** -0.5, 0.125, ((0, 8), (2, 4)))
    w_up = scatter_about(key_of[9], (EXPERTS, D, FF_E), D ** -0.5, 0.125, ((0, 8), (2, 4)))
    w_down = scatter_about(key_of[10], (EXPERTS, FF_E, D), FF_E ** -0.5, 0.1875, ((0, 8), (1, 4)))
    return {"pool_in": pool_in, "w_pool": w_pool, "pool_scale": pool_scale, "w_out": w_out, "expert_in": expert_in, "ffn_gain": ffn_gain, "routes": routes, "route_weight": route_weight, "w_gate": w_gate, "w_up": w_up, "w_down": w_down}


EPS = 0.05

def window_sizes(width):
    group_of = jnp.arange(width) // GDIM
    level = group_of % 4
    return jnp.where(level == 0, 2.0, jnp.where(level == 1, 4.0, jnp.where(level == 2, 8.0, 16.0))).astype(jnp.float32)

def pooled_rows(extended, positions):
    extent = extended.shape[0] - (WMAX - 1)
    window = window_sizes(extended.shape[1])
    running = jnp.zeros((extent, extended.shape[1]), jnp.float32)
    picked = running
    for offset in range(WMAX):
        running = running + extended[WMAX - 1 - offset:WMAX - 1 - offset + extent]
        if offset + 1 in (2, 4, 8, 16):
            picked = jnp.where(window[None, :] == offset + 1, running, picked)
    counted = jnp.minimum(positions[:, None] + 1.0, window[None, :])
    return (picked / counted - extended[WMAX - 1:]).astype(jnp.bfloat16)

def reference(pool_in, w_pool, pool_scale, w_out, expert_in, ffn_gain, routes, route_weight, w_gate, w_up, w_down):
    extended = jnp.pad(pool_in.astype(jnp.float32), ((WMAX - 1, 0), (0, 0)))
    positions = jnp.arange(TOKENS_A).astype(jnp.float32)
    pooled = pooled_rows(extended, positions)
    grouped = jnp.einsum('lgc,gcd->lgd', pooled.reshape(TOKENS_A, GROUPS, GDIM).astype(jnp.float32), w_pool.astype(jnp.float32))
    scaled = (grouped.reshape(TOKENS_A, PW) * pool_scale).astype(jnp.bfloat16)
    mixer_out = jnp.dot(scaled, w_out, preferred_element_type=jnp.float32).astype(jnp.bfloat16)
    features = expert_in.astype(jnp.float32)
    inverse = lax.rsqrt(lax.optimization_barrier(jnp.mean(features * features, axis=-1, keepdims=True)) + EPS)
    normed = (features * inverse * ffn_gain).astype(jnp.bfloat16)
    flat_ids = routes.reshape(-1).astype(jnp.int32)
    flat_weights = route_weight.reshape(-1)
    most_rows = N_EP * N_TP * CAP
    quarter = FF_E // N_TP

    def one_expert(expert, running):
        chosen = flat_ids == expert
        slot_index = jnp.nonzero(chosen, size=most_rows, fill_value=0)[0].astype(jnp.int32)
        filled = jnp.arange(most_rows) < jnp.sum(chosen.astype(jnp.int32))
        token_rows = (slot_index // K).astype(jnp.int32)
        picked_rows = normed[token_rows]
        gate_val = jnp.dot(picked_rows, w_gate[expert], preferred_element_type=jnp.float32)
        up_val = jnp.dot(picked_rows, w_up[expert], preferred_element_type=jnp.float32)
        hidden = (jax.nn.silu(gate_val) * up_val).astype(jnp.bfloat16)
        down_rows = w_down[expert]
        summed = jnp.zeros((most_rows, D), jnp.float32)
        for block in range(N_TP):
            partial_val = jnp.dot(hidden[:, block * quarter:(block + 1) * quarter], down_rows[block * quarter:(block + 1) * quarter], preferred_element_type=jnp.float32).astype(jnp.bfloat16)
            partial_val = lax.optimization_barrier(partial_val)
            summed = summed + partial_val.astype(jnp.float32)
        expert_val = summed.astype(jnp.bfloat16)
        weights = jnp.where(filled, flat_weights[slot_index], jnp.zeros((), jnp.float32))
        return running.at[token_rows].add(weights[:, None] * expert_val.astype(jnp.float32))
    combined = lax.fori_loop(0, EXPERTS, one_expert, jnp.zeros((TOKENS_B, D), jnp.float32))
    return (mixer_out, combined.astype(jnp.bfloat16))
```

```python
import functools

import jax
import jax.numpy as jnp
from jax import lax
from jax.experimental import pallas as pl
from jax.experimental.pallas import tpu as pltpu
from jax.sharding import PartitionSpec as P

GDIM = 128
WMAX = 16
K = 2
EPS = 0.05
MESH = pl.DeviceIdType.MESH
F32 = jnp.float32
BF16 = jnp.bfloat16
LANES = 128


def dot(a, b):
    return jnp.dot(a, b, preferred_element_type=F32)


def kernel(
    dims,
    routes_ref,
    weight_ref,
    gain_ref,
    scale_ref,
    wpool_hbm,
    pool_hbm,
    wout_hbm,
    rows_hbm,
    gate_hbm,
    up_hbm,
    down_hbm,
    mixer_v,
    expert_v,
    wpool_ref,
    pool_v,
    halo_v,
    wout_v,
    scaled_v,
    mine_v,
    normed_v,
    outgoing,
    arrived,
    gate_all,
    up_all,
    gate_sum,
    up_sum,
    hidden,
    down_all,
    result,
    returned,
    relay_in,
    relay_out,
    dense,
    near_routes,
    near_weights,
    merge_high,
    merge_low,
    local_sem,
    far_s,
    far_r,
    near_s,
    near_r,
    relay_s,
    relay_r,
    go_s,
    go_r,
    back_s,
    back_r,
    group_r,
    dense_s,
    dense_r,
    names_s,
    names_r,
    halo_s,
    halo_r,
):
    ep_n, tp_n, cap, gate_n, down_n = dims
    me = lax.axis_index("ep")
    own = lax.axis_index("tp")
    near = own + 1 - 2 * (own % 2)
    far = (own + tp_n // 2) % tp_n
    index = me * tp_n + own
    total = ep_n * tp_n
    after = (index + 1) % total
    before = (index + total - 1) % total
    block_rows, width = mine_v.shape
    slots = ep_n * cap
    local = gate_hbm.shape[2]
    deep = width // gate_n
    part = width // down_n

    half = ep_n // 2
    plane = ep_n // 4
    upper = me // half
    first = upper * half
    other = half - first
    mine = me - first
    relays = half - plane + upper * plane
    is_relay = (me >= half - plane) & (me < half + plane)
    my_relay = half - upper * plane + me % plane
    my_turn = mine // plane

    def partner(i):
        return (me + ep_n // 2 + ((i + 1) // 2) * (1 - 2 * (i % 2))) % ep_n

    barrier = pltpu.get_barrier_semaphore()

    def greet(i, _):
        pl.semaphore_signal(barrier, inc=1, device_id=(partner(i), own), device_id_type=MESH)
        return 0

    lax.fori_loop(0, ep_n - 1, greet, 0)
    for there in (
        (me, near),
        (me, far),
        (after // tp_n, after % tp_n),
        (before // tp_n, before % tp_n),
    ):
        pl.semaphore_signal(barrier, inc=1, device_id=there, device_id_type=MESH)

    def down_cols(c):
        return pl.ds(pl.multiple_of(c * part, LANES), part)

    loads = [
        pltpu.make_async_copy(
            rows_hbm.at[pl.ds(own * block_rows, block_rows)], mine_v, local_sem.at[0]
        ),
        pltpu.make_async_copy(pool_hbm, pool_v, local_sem.at[1]),
        pltpu.make_async_copy(wout_hbm, wout_v, local_sem.at[2]),
        pltpu.make_async_copy(gate_hbm.at[0], gate_all.at[0], local_sem.at[3]),
        pltpu.make_async_copy(up_hbm.at[0], up_all.at[0], local_sem.at[4]),
        pltpu.make_async_copy(wpool_hbm, wpool_ref, local_sem.at[5]),
    ]
    for load in loads:
        load.start()

    def own_down(c):
        return pltpu.make_async_copy(
            down_hbm.at[0, :, down_cols(c)], down_all.at[c, 0:local], local_sem.at[7 + c]
        )

    pl.semaphore_wait(barrier, ep_n + 3)

    def to_far(src, dst, at):
        return pltpu.make_async_remote_copy(
            src_ref=src,
            dst_ref=dst,
            send_sem=far_s.at[at],
            recv_sem=far_r.at[at],
            device_id=(me, far),
            device_id_type=MESH,
        )

    def to_near(src, dst, at, send, recv):
        return pltpu.make_async_remote_copy(
            src_ref=src,
            dst_ref=dst,
            send_sem=send.at[at],
            recv_sem=recv.at[at],
            device_id=(me, near),
            device_id_type=MESH,
        )

    def far_gate(k):
        some = pl.ds(k * deep, deep)
        return (
            to_far(gate_hbm.at[0, some], gate_all.at[2, some], 2 * k),
            to_far(up_hbm.at[0, some], up_all.at[2, some], 2 * k + 1),
        )

    def relay_gate(k):
        some = pl.ds(k * deep, deep)
        return (
            to_near(gate_all.at[2, some], gate_all.at[3, some], 2 * k, relay_s, relay_r),
            to_near(up_all.at[2, some], up_all.at[3, some], 2 * k + 1, relay_s, relay_r),
        )

    def far_down(c):
        return to_far(
            down_hbm.at[0, :, down_cols(c)],
            down_all.at[c, 2 * local : 3 * local],
            2 * gate_n + c,
        )

    def relay_down(c):
        return to_near(
            down_all.at[c, 2 * local : 3 * local],
            down_all.at[c, 3 * local : 4 * local],
            2 * gate_n + c,
            relay_s,
            relay_r,
        )

    def near_down(c):
        return to_near(
            down_hbm.at[0, :, down_cols(c)],
            down_all.at[c, local : 2 * local],
            2 + c,
            near_s,
            near_r,
        )

    near_gate = (
        to_near(gate_hbm.at[0], gate_all.at[1], 0, near_s, near_r),
        to_near(up_hbm.at[0], up_all.at[1], 1, near_s, near_r),
    )
    rows_here = pool_v.shape[0]
    halo = pltpu.make_async_remote_copy(
        src_ref=pool_hbm.at[rows_here - WMAX :],
        dst_ref=halo_v,
        send_sem=halo_s,
        recv_sem=halo_r,
        device_id=(after // tp_n, after % tp_n),
        device_id_type=MESH,
    )
    halo.start()

    def to_relay(src, dst, at):
        return pltpu.make_async_remote_copy(
            src_ref=src.at[:, pl.ds(pl.multiple_of(own * block_rows, block_rows), block_rows)],
            dst_ref=dst,
            send_sem=names_s.at[at],
            recv_sem=names_r.at[at, my_turn],
            device_id=(my_relay, own),
            device_id_type=MESH,
        )

    to_relay(routes_ref, near_routes.at[my_turn], 0).start()
    to_relay(weight_ref, near_weights.at[my_turn], 1).start()
    for k in range(gate_n):
        for copy in far_gate(k):
            copy.start()

    def start_far_down(c, _):
        far_down(c).start()
        return 0

    lax.fori_loop(0, down_n, start_far_down, 0)

    block = pl.ds(pl.multiple_of(own * block_rows, block_rows), block_rows)
    tall = max(ep_n, 16)
    expert_of = lax.broadcasted_iota(jnp.int32, (tall, block_rows), 0)
    earlier = (
        lax.broadcasted_iota(jnp.int32, (block_rows, block_rows), 0)
        < lax.broadcasted_iota(jnp.int32, (block_rows, block_rows), 1)
    )
    earlier = jnp.where(earlier, 1.0, 0.0).astype(BF16)

    def places(routes):
        names = [expert_of == routes[j : j + 1] for j in range(K)]
        named = jnp.where(names[0] | names[1], 1.0, 0.0).astype(BF16)
        rank = dot(named, earlier)
        return [
            routes[j : j + 1] * cap
            + jnp.sum(jnp.where(names[j], rank, 0.0), axis=0, keepdims=True).astype(jnp.int32)
            for j in range(K)
        ]

    def set_merge(at, place, weights):
        slot_of = first * cap + lax.broadcasted_iota(jnp.int32, (half * cap, block_rows), 0)
        merged = jnp.zeros((half * cap, block_rows), F32)
        for j in range(K):
            merged = merged + jnp.where(slot_of == place[j], weights[j : j + 1], 0.0)
        merge = merged.T
        high = merge.astype(BF16)
        merge_high[at] = high
        merge_low[at] = (merge - high.astype(F32)).astype(BF16)

    place = places(routes_ref[:, block])
    slot_of = lax.broadcasted_iota(jnp.int32, (slots, block_rows), 0)
    spread = jnp.zeros((slots, block_rows), F32)
    for j in range(K):
        spread = spread + jnp.where(slot_of == place[j], 1.0, 0.0)
    spread = spread.astype(BF16)

    loads[0].wait()
    features = mine_v[...].astype(F32)
    inverse = lax.rsqrt(jnp.mean(features * features, axis=-1, keepdims=True) + EPS)
    normed_v[...] = (features * inverse * gain_ref[...]).astype(BF16)

    step = 512

    def spread_cols(i, _):
        cols = pl.ds(pl.multiple_of(i * step, step), step)
        rows = dot(spread, normed_v[:, cols]).astype(BF16)
        outgoing[:, :, cols] = rows.reshape(ep_n, cap, step)
        return 0

    lax.fori_loop(0, width // step, spread_cols, 0)

    def go(peer, slot):
        return pltpu.make_async_remote_copy(
            src_ref=outgoing.at[peer],
            dst_ref=arrived.at[slot],
            send_sem=go_s.at[peer],
            recv_sem=go_r.at[slot],
            device_id=(peer, own),
            device_id_type=MESH,
        )

    def start_go(i, _):
        go(partner(i), me).start()
        return 0

    lax.fori_loop(0, ep_n - 1, start_go, 0)
    arrived[me] = outgoing[me]

    for copy in near_gate:
        copy.start()

    def start_near_down(c, _):
        near_down(c).start()
        own_down(c).start()
        return 0

    lax.fori_loop(0, down_n, start_near_down, 0)

    set_merge(0, place, weight_ref[:, block])

    loads[1].wait()
    loads[5].wait()
    halo.wait_recv()
    position = (
        index * rows_here + lax.broadcasted_iota(jnp.int32, (rows_here, GDIM), 0)
    ).astype(F32)
    for g in range(wpool_ref.shape[0]):
        window = 2 ** (1 + g % 4)
        cols = slice(g * GDIM, (g + 1) * GDIM)
        head = jnp.where(index > 0, halo_v[:, cols].astype(F32), 0.0)
        here = pool_v[:, cols].astype(F32)
        running = jnp.concatenate([head, here], axis=0)
        shift = 1
        while shift < window:
            running = running + pltpu.roll(running, shift, 0)
            shift *= 2
        counted = jnp.minimum(position + 1.0, float(window))
        pooled = (running[WMAX:] / counted - here).astype(BF16)
        scaled_v[:, cols] = (dot(pooled, wpool_ref[g]) * scale_ref[:, cols]).astype(BF16)
    loads[2].wait()

    def mix_cols(i, _):
        cols = pl.ds(pl.multiple_of(i * step, step), step)
        mixer_v[:, cols] = dot(scaled_v[...], wout_v[:, cols]).astype(BF16)
        return 0

    lax.fori_loop(0, width // step, mix_cols, 0)

    @pl.when(is_relay)
    def _():
        for k in range(2):
            for at, held in enumerate((near_routes, near_weights)):
                pltpu.make_async_remote_copy(
                    src_ref=held.at[k],
                    dst_ref=held.at[k],
                    send_sem=names_s.at[at],
                    recv_sem=names_r.at[at, k],
                    device_id=(my_relay, own),
                    device_id_type=MESH,
                ).wait_recv()
            set_merge(1 + k, places(near_routes[k]), near_weights[k])

    def activate(slot, gate_val, up_val):
        value = gate_val / (1.0 + jnp.exp(-gate_val)) * up_val
        cols = pl.ds(pl.multiple_of(slot * local, LANES), local)
        hidden[:, cols] = value.astype(BF16)

    def relay(k):
        for copy in far_gate(k):
            copy.wait_recv()
        for copy in relay_gate(k):
            copy.start()

    for k in range(gate_n - 1):
        relay(k)
    loads[3].wait()
    loads[4].wait()
    for copy in near_gate:
        copy.wait_recv()

    def wait_go(i, _):
        go(me, partner(i)).wait_recv()
        return 0

    lax.fori_loop(0, ep_n - 1, wait_go, 0)

    def gated_slot(slot, _):
        rows = arrived[...].reshape(slots, width)
        activate(slot, dot(rows, gate_all[slot]), dot(rows, up_all[slot]))
        return 0

    lax.fori_loop(0, 2, gated_slot, 0)
    for k in range(gate_n - 1):
        for copy in relay_gate(k):
            copy.wait_recv()
    most = (gate_n - 1) * deep

    def most_slot(slot, _):
        rows = arrived[:, :, :most].reshape(slots, most)
        gate_sum[slot - 2] = dot(rows, gate_all[slot, :most])
        up_sum[slot - 2] = dot(rows, up_all[slot, :most])
        return 0

    lax.fori_loop(2, 4, most_slot, 0)
    relay(gate_n - 1)

    def last_slot(slot, _):
        @pl.when(slot == 3)
        def _():
            for copy in relay_gate(gate_n - 1):
                copy.wait_recv()

        rows = arrived[:, :, most:].reshape(slots, deep)
        activate(
            slot,
            gate_sum[slot - 2] + dot(rows, gate_all[slot, most:]),
            up_sum[slot - 2] + dot(rows, up_all[slot, most:]),
        )
        return 0

    lax.fori_loop(2, 4, last_slot, 0)

    def peer_of(i):
        return (mine + 1 + i) % half

    def back(c, peer, slot):
        return pltpu.make_async_remote_copy(
            src_ref=result.at[c, first + peer],
            dst_ref=returned.at[c, slot],
            send_sem=back_s.at[c, first + peer],
            recv_sem=back_r.at[c, slot],
            device_id=(first + peer, own),
            device_id_type=MESH,
        )

    def group(c, i, slot):
        return pltpu.make_async_remote_copy(
            src_ref=result.at[c, other + i],
            dst_ref=relay_in.at[c, i // plane, slot],
            send_sem=back_s.at[c, other + i],
            recv_sem=group_r.at[c, i // plane, slot],
            device_id=(relays + i % plane, own),
            device_id_type=MESH,
        )

    def dense_to(c, k):
        return pltpu.make_async_remote_copy(
            src_ref=relay_out.at[c, k],
            dst_ref=dense.at[c],
            send_sem=dense_s.at[c, k],
            recv_sem=dense_r.at[c],
            device_id=(other + k * plane + me % plane, own),
            device_id_type=MESH,
        )

    def weighed(at, values):
        return dot(merge_high[at], values) + dot(merge_low[at], values)

    def pass_on(c):
        for k in range(2):

            def wait_group(i, _):
                group(c, k * plane + me % plane, peer_of(i)).wait_recv()
                return 0

            lax.fori_loop(0, half - 1, wait_group, 0)
            values = relay_in[c, k].reshape(half * cap, part)
            relay_out[c, k] = weighed(1 + k, values).astype(BF16)
            dense_to(c, k).start()

    def down_part(c, _):
        far_down(c).wait_recv()
        relay_down(c).start()
        own_down(c).wait()
        near_down(c).wait_recv()
        relay_down(c).wait_recv()
        value = dot(hidden[...], down_all[c]).astype(BF16).reshape(ep_n, cap, part)
        result[c] = value

        def start_group(i, _):
            @pl.when(relays + i % plane != me)
            def _():
                group(c, i, mine).start()

            return 0

        lax.fori_loop(0, half, start_group, 0)

        def start_back(i, _):
            back(c, peer_of(i), mine).start()
            return 0

        lax.fori_loop(0, half - 1, start_back, 0)
        returned[c, mine] = result[c, me]

        @pl.when(is_relay)
        def _():
            for k in range(2):
                relay_in[c, k, mine] = result[c, other + k * plane + me % plane]

            @pl.when(c > 0)
            def _():
                pass_on(c - 1)

        return 0

    lax.fori_loop(0, down_n, down_part, 0)

    @pl.when(is_relay)
    def _():
        pass_on(down_n - 1)

    def combine(c, _):
        def wait_back(i, _):
            back(c, mine, peer_of(i)).wait_recv()
            return 0

        lax.fori_loop(0, half - 1, wait_back, 0)
        pltpu.make_async_remote_copy(
            src_ref=dense.at[c],
            dst_ref=dense.at[c],
            send_sem=dense_s.at[c, 0],
            recv_sem=dense_r.at[c],
            device_id=(my_relay, own),
            device_id_type=MESH,
        ).wait_recv()
        values = returned[c].reshape(half * cap, part)
        expert_v[:, down_cols(c)] = (weighed(0, values) + dense[c].astype(F32)).astype(BF16)
        return 0

    lax.fori_loop(0, down_n, combine, 0)

    halo.wait_send()
    to_relay(routes_ref, near_routes.at[my_turn], 0).wait_send()
    to_relay(weight_ref, near_weights.at[my_turn], 1).wait_send()
    for k in range(gate_n):
        for copy in far_gate(k) + relay_gate(k):
            copy.wait_send()
    for copy in near_gate:
        copy.wait_send()

    def end_down(c, _):
        far_down(c).wait_send()
        relay_down(c).wait_send()
        near_down(c).wait_send()

        def end_back(i, _):
            back(c, peer_of(i), mine).wait_send()
            return 0

        lax.fori_loop(0, half - 1, end_back, 0)

        def end_group(i, _):
            @pl.when(relays + i % plane != me)
            def _():
                group(c, i, mine).wait_send()

            return 0

        lax.fori_loop(0, half, end_group, 0)

        @pl.when(is_relay)
        def _():
            for k in range(2):
                dense_to(c, k).wait_send()

        return 0

    lax.fori_loop(0, down_n, end_down, 0)

    def end_go(i, _):
        go(partner(i), me).wait_send()
        return 0

    lax.fori_loop(0, ep_n - 1, end_go, 0)


def on_device(
    pool_in,
    w_pool,
    pool_scale,
    w_out,
    expert_in,
    ffn_gain,
    routes,
    route_weight,
    w_gate,
    w_up,
    w_down,
):
    ep_n = lax.axis_size("ep")
    tp_n = lax.axis_size("tp")
    assert tp_n == 4 and ep_n % 4 == 0 and w_gate.shape[0] == 1
    half = ep_n // 2
    block_rows = routes.shape[0] // tp_n
    capacity = 3 * block_rows * K // (2 * ep_n)
    cap = -(-capacity // 16) * 16
    width = expert_in.shape[1]
    rows_here, pool_width = pool_in.shape
    local = w_gate.shape[2]
    slots = ep_n * cap
    down_n = 8
    part = width // down_n
    gate_n = 4
    vmem = pl.BlockSpec(memory_space=pltpu.VMEM)
    hbm = pl.BlockSpec(memory_space=pl.ANY)
    dma = pltpu.SemaphoreType.DMA
    return pl.pallas_call(
        functools.partial(kernel, (ep_n, tp_n, cap, gate_n, down_n)),
        out_shape=(
            pltpu.VMEM((rows_here, width), BF16),
            pltpu.VMEM((block_rows, width), BF16),
        ),
        in_specs=[vmem] * 4 + [hbm] * 7,
        out_specs=(vmem, vmem),
        scratch_shapes=[
            pltpu.VMEM(w_pool.shape, BF16),
            pltpu.VMEM((rows_here, pool_width), BF16),
            pltpu.VMEM((WMAX, pool_width), BF16),
            pltpu.VMEM((pool_width, width), BF16),
            pltpu.VMEM((rows_here, pool_width), BF16),
            pltpu.VMEM((block_rows, width), BF16),
            pltpu.VMEM((block_rows, width), BF16),
            pltpu.VMEM((ep_n, cap, width), BF16),
            pltpu.VMEM((ep_n, cap, width), BF16),
            pltpu.VMEM((tp_n, width, local), BF16),
            pltpu.VMEM((tp_n, width, local), BF16),
            pltpu.VMEM((2, slots, local), F32),
            pltpu.VMEM((2, slots, local), F32),
            pltpu.VMEM((slots, tp_n * local), BF16),
            pltpu.VMEM((down_n, tp_n * local, part), BF16),
            pltpu.VMEM((down_n, ep_n, cap, part), BF16),
            pltpu.VMEM((down_n, half, cap, part), BF16),
            pltpu.VMEM((down_n, 2, half, cap, part), BF16),
            pltpu.VMEM((down_n, 2, block_rows, part), BF16),
            pltpu.VMEM((down_n, block_rows, part), BF16),
            pltpu.VMEM((2, K, block_rows), jnp.int32),
            pltpu.VMEM((2, K, block_rows), F32),
            pltpu.VMEM((3, block_rows, half * cap), BF16),
            pltpu.VMEM((3, block_rows, half * cap), BF16),
            dma((7 + down_n,)),
            dma((2 * gate_n + down_n,)),
            dma((2 * gate_n + down_n,)),
            dma((2 + down_n,)),
            dma((2 + down_n,)),
            dma((2 * gate_n + down_n,)),
            dma((2 * gate_n + down_n,)),
            dma((ep_n,)),
            dma((ep_n,)),
            dma((down_n, ep_n)),
            dma((down_n, half)),
            dma((down_n, 2, half)),
            dma((down_n, 2)),
            dma((down_n,)),
            dma((2,)),
            dma((2, 2)),
            dma,
            dma,
        ],
        compiler_params=pltpu.CompilerParams(
            collective_id=0, has_side_effects=True, vmem_limit_bytes=60 * 1024 * 1024
        ),
    )(
        routes.T,
        route_weight.T,
        ffn_gain.reshape(1, -1),
        pool_scale.reshape(1, -1),
        w_pool,
        pool_in,
        w_out,
        expert_in,
        w_gate,
        w_up,
        w_down,
    )


def solution(mesh):
    placed = (
        P(("ep", "tp"), None),
        P(),
        P(),
        P(),
        P("ep", None),
        P(),
        P("ep", None),
        P("ep", None),
        P("ep", None, "tp"),
        P("ep", None, "tp"),
        P("ep", "tp", None),
    )
    return jax.shard_map(
        on_device,
        mesh=mesh,
        in_specs=placed,
        out_specs=(P(("ep", "tp"), None), P(("ep", "tp"), None)),
        check_vma=False,
    )
```

```python
import functools

import jax
import jax.numpy as jnp
from jax import lax
from jax.experimental import pallas as pl
from jax.experimental.pallas import tpu as pltpu
from jax.sharding import PartitionSpec as P

GDIM = 128
WMAX = 16
K = 2
EPS = 0.05
MESH = pl.DeviceIdType.MESH
F32 = jnp.float32
BF16 = jnp.bfloat16
LANES = 128


def dot(a, b):
    return jnp.dot(a, b, preferred_element_type=F32)


def kernel(
    dims,
    routes_ref,
    weight_ref,
    gain_ref,
    scale_ref,
    wpool_hbm,
    pool_hbm,
    wout_hbm,
    rows_hbm,
    gate_hbm,
    up_hbm,
    down_hbm,
    mixer_v,
    expert_v,
    wpool_ref,
    pool_v,
    halo_v,
    wout_v,
    scaled_v,
    mine_v,
    normed_v,
    outgoing,
    arrived,
    gate_all,
    up_all,
    gate_sum,
    up_sum,
    hidden,
    down_all,
    result,
    returned,
    relay_in,
    relay_out,
    dense,
    near_routes,
    near_weights,
    merge_high,
    merge_low,
    local_sem,
    far_s,
    far_r,
    near_s,
    near_r,
    relay_s,
    relay_r,
    go_s,
    go_r,
    back_s,
    back_r,
    group_r,
    dense_s,
    dense_r,
    names_s,
    names_r,
    halo_s,
    halo_r,
    hello,
    ready,
):
    ep_n, tp_n, cap, gate_n, down_n = dims
    me = lax.axis_index("ep")
    own = lax.axis_index("tp")
    near = own + 1 - 2 * (own % 2)
    far = (own + tp_n // 2) % tp_n
    index = me * tp_n + own
    total = ep_n * tp_n
    after = (index + 1) % total
    before = (index + total - 1) % total
    block_rows, width = mine_v.shape
    slots = ep_n * cap
    local = gate_hbm.shape[2]
    deep = width // gate_n
    part = width // down_n

    half = ep_n // 2
    plane = ep_n // 4
    upper = me // half
    first = upper * half
    other = half - first
    mine = me - first
    relays = half - plane + upper * plane
    is_relay = (me >= half - plane) & (me < half + plane)
    my_relay = half - upper * plane + me % plane
    my_turn = mine // plane

    def partner(i):
        return (me + ep_n // 2 + ((i + 1) // 2) * (1 - 2 * (i % 2))) % ep_n

    barrier = pltpu.get_barrier_semaphore()

    lead = own < tp_n // 2
    follow = own >= tp_n // 2

    @pl.when(lead)
    def _():
        pl.semaphore_signal(barrier, inc=1, device_id=(me, far), device_id_type=MESH)

    def down_cols(c):
        return pl.ds(pl.multiple_of(c * part, LANES), part)

    loads = [
        pltpu.make_async_copy(
            rows_hbm.at[pl.ds(own * block_rows, block_rows)], mine_v, local_sem.at[0]
        ),
        pltpu.make_async_copy(pool_hbm, pool_v, local_sem.at[1]),
        pltpu.make_async_copy(wout_hbm, wout_v, local_sem.at[2]),
        pltpu.make_async_copy(gate_hbm.at[0], gate_all.at[0], local_sem.at[3]),
        pltpu.make_async_copy(up_hbm.at[0], up_all.at[0], local_sem.at[4]),
        pltpu.make_async_copy(wpool_hbm, wpool_ref, local_sem.at[5]),
    ]
    for load in loads:
        load.start()

    def own_down(c):
        return pltpu.make_async_copy(
            down_hbm.at[0, :, down_cols(c)], down_all.at[c, 0:local], local_sem.at[7 + c]
        )

    @pl.when(follow)
    def _():
        pl.semaphore_wait(barrier, 1)
        pl.semaphore_signal(hello, inc=1, device_id=(me, far), device_id_type=MESH)

    @pl.when(lead)
    def _():
        pl.semaphore_wait(hello, 1)

    def to_far(src, dst, at):
        return pltpu.make_async_remote_copy(
            src_ref=src,
            dst_ref=dst,
            send_sem=far_s.at[at],
            recv_sem=far_r.at[at],
            device_id=(me, far),
            device_id_type=MESH,
        )

    def to_near(src, dst, at, send, recv):
        return pltpu.make_async_remote_copy(
            src_ref=src,
            dst_ref=dst,
            send_sem=send.at[at],
            recv_sem=recv.at[at],
            device_id=(me, near),
            device_id_type=MESH,
        )

    def far_gate(k):
        some = pl.ds(k * deep, deep)
        return (
            to_far(gate_hbm.at[0, some], gate_all.at[2, some], 2 * k),
            to_far(up_hbm.at[0, some], up_all.at[2, some], 2 * k + 1),
        )

    def relay_gate(k):
        some = pl.ds(k * deep, deep)
        return (
            to_near(gate_all.at[2, some], gate_all.at[3, some], 2 * k, relay_s, relay_r),
            to_near(up_all.at[2, some], up_all.at[3, some], 2 * k + 1, relay_s, relay_r),
        )

    def far_down(c):
        return to_far(
            down_hbm.at[0, :, down_cols(c)],
            down_all.at[c, 2 * local : 3 * local],
            2 * gate_n + c,
        )

    def relay_down(c):
        return to_near(
            down_all.at[c, 2 * local : 3 * local],
            down_all.at[c, 3 * local : 4 * local],
            2 * gate_n + c,
            relay_s,
            relay_r,
        )

    def near_down(c):
        return to_near(
            down_hbm.at[0, :, down_cols(c)],
            down_all.at[c, local : 2 * local],
            2 + c,
            near_s,
            near_r,
        )

    near_gate = (
        to_near(gate_hbm.at[0], gate_all.at[1], 0, near_s, near_r),
        to_near(up_hbm.at[0], up_all.at[1], 1, near_s, near_r),
    )
    rows_here = pool_v.shape[0]
    halo = pltpu.make_async_remote_copy(
        src_ref=pool_hbm.at[rows_here - WMAX :],
        dst_ref=halo_v,
        send_sem=halo_s,
        recv_sem=halo_r,
        device_id=(after // tp_n, after % tp_n),
        device_id_type=MESH,
    )

    def to_relay(src, dst, at):
        return pltpu.make_async_remote_copy(
            src_ref=src.at[:, pl.ds(pl.multiple_of(own * block_rows, block_rows), block_rows)],
            dst_ref=dst,
            send_sem=names_s.at[at],
            recv_sem=names_r.at[at, my_turn],
            device_id=(my_relay, own),
            device_id_type=MESH,
        )

    ahead = [copy for k in range(gate_n) for copy in far_gate(k)]
    for copy in ahead[:3]:
        copy.start()

    @pl.when(follow)
    def _():
        for copy in ahead[3:4]:
            copy.start()

    @pl.when(lead)
    def _():
        def greet(i, _):
            peer = (me + 1 + i) % ep_n
            pl.semaphore_signal(barrier, inc=1, device_id=(peer, own), device_id_type=MESH)
            return 0

        lax.fori_loop(0, ep_n - 1, greet, 0)
        beside = (me + ep_n - 1 + 2 * (own % 2)) % ep_n
        for there in ((me, near), (beside, near)):
            pl.semaphore_signal(barrier, inc=1, device_id=there, device_id_type=MESH)


    block = pl.ds(pl.multiple_of(own * block_rows, block_rows), block_rows)
    tall = max(ep_n, 16)
    expert_of = lax.broadcasted_iota(jnp.int32, (tall, block_rows), 0)
    earlier = (
        lax.broadcasted_iota(jnp.int32, (block_rows, block_rows), 0)
        < lax.broadcasted_iota(jnp.int32, (block_rows, block_rows), 1)
    )
    earlier = jnp.where(earlier, 1.0, 0.0).astype(BF16)

    def places(routes):
        names = [expert_of == routes[j : j + 1] for j in range(K)]
        named = jnp.where(names[0] | names[1], 1.0, 0.0).astype(BF16)
        rank = dot(named, earlier)
        return [
            routes[j : j + 1] * cap
            + jnp.sum(jnp.where(names[j], rank, 0.0), axis=0, keepdims=True).astype(jnp.int32)
            for j in range(K)
        ]

    def set_merge(at, place, weights):
        slot_of = first * cap + lax.broadcasted_iota(jnp.int32, (half * cap, block_rows), 0)
        merged = jnp.zeros((half * cap, block_rows), F32)
        for j in range(K):
            merged = merged + jnp.where(slot_of == place[j], weights[j : j + 1], 0.0)
        merge = merged.T
        high = merge.astype(BF16)
        merge_high[at] = high
        merge_low[at] = (merge - high.astype(F32)).astype(BF16)

    place = places(routes_ref[:, block])
    slot_of = lax.broadcasted_iota(jnp.int32, (slots, block_rows), 0)
    spread = jnp.zeros((slots, block_rows), F32)
    for j in range(K):
        spread = spread + jnp.where(slot_of == place[j], 1.0, 0.0)
    spread = spread.astype(BF16)

    @pl.when(lead)
    def _():
        pl.semaphore_wait(barrier, ep_n + 1)
        pl.semaphore_signal(ready, inc=1, device_id=(me, far), device_id_type=MESH)

    @pl.when(follow)
    def _():
        pl.semaphore_wait(ready, 1)

    halo.start()

    @pl.when(lead)
    def _():
        for copy in ahead[3:4]:
            copy.start()

    for copy in ahead[4:]:
        copy.start()

    def start_far_down(c, _):
        far_down(c).start()
        return 0

    lax.fori_loop(0, down_n, start_far_down, 0)
    to_relay(routes_ref, near_routes.at[my_turn], 0).start()
    to_relay(weight_ref, near_weights.at[my_turn], 1).start()

    loads[0].wait()
    features = mine_v[...].astype(F32)
    inverse = lax.rsqrt(jnp.mean(features * features, axis=-1, keepdims=True) + EPS)
    normed_v[...] = (features * inverse * gain_ref[...]).astype(BF16)

    step = 512
    lag = 2

    def spread_cols(i, _):
        cols = pl.ds(pl.multiple_of(i * step, step), step)
        rows = dot(spread, normed_v[:, cols]).astype(BF16)
        outgoing[:, :, cols] = rows.reshape(ep_n, cap, step)
        return 0

    lax.fori_loop(0, width // step, spread_cols, 0)

    def go(peer, slot):
        return pltpu.make_async_remote_copy(
            src_ref=outgoing.at[peer],
            dst_ref=arrived.at[slot],
            send_sem=go_s.at[peer],
            recv_sem=go_r.at[slot],
            device_id=(peer, own),
            device_id_type=MESH,
        )

    def start_go(i, _):
        go(partner(i), me).start()
        return 0

    lax.fori_loop(0, ep_n - 1, start_go, 0)
    arrived[me] = outgoing[me]

    for copy in near_gate:
        copy.start()

    def start_near_down(c, _):
        near_down(c).start()
        own_down(c).start()
        return 0

    lax.fori_loop(0, down_n, start_near_down, 0)

    set_merge(0, place, weight_ref[:, block])

    loads[1].wait()
    loads[5].wait()
    halo.wait_recv()
    position = (
        index * rows_here + lax.broadcasted_iota(jnp.int32, (rows_here, GDIM), 0)
    ).astype(F32)
    for g in range(wpool_ref.shape[0]):
        window = 2 ** (1 + g % 4)
        cols = slice(g * GDIM, (g + 1) * GDIM)
        head = jnp.where(index > 0, halo_v[:, cols].astype(F32), 0.0)
        here = pool_v[:, cols].astype(F32)
        running = jnp.concatenate([head, here], axis=0)
        shift = 1
        while shift < window:
            running = running + pltpu.roll(running, shift, 0)
            shift *= 2
        counted = jnp.minimum(position + 1.0, float(window))
        pooled = (running[WMAX:] / counted - here).astype(BF16)
        scaled_v[:, cols] = (dot(pooled, wpool_ref[g]) * scale_ref[:, cols]).astype(BF16)
    loads[2].wait()

    def mix_cols(i, _):
        cols = pl.ds(pl.multiple_of(i * step, step), step)
        mixer_v[:, cols] = dot(scaled_v[...], wout_v[:, cols]).astype(BF16)
        return 0

    lax.fori_loop(0, width // step, mix_cols, 0)

    @pl.when(is_relay)
    def _():
        for k in range(2):
            for at, held in enumerate((near_routes, near_weights)):
                pltpu.make_async_remote_copy(
                    src_ref=held.at[k],
                    dst_ref=held.at[k],
                    send_sem=names_s.at[at],
                    recv_sem=names_r.at[at, k],
                    device_id=(my_relay, own),
                    device_id_type=MESH,
                ).wait_recv()
            set_merge(1 + k, places(near_routes[k]), near_weights[k])

    def activate(slot, gate_val, up_val):
        value = gate_val / (1.0 + jnp.exp(-gate_val)) * up_val
        cols = pl.ds(pl.multiple_of(slot * local, LANES), local)
        hidden[:, cols] = value.astype(BF16)

    def relay(k):
        for copy in far_gate(k):
            copy.wait_recv()
        for copy in relay_gate(k):
            copy.start()

    for k in range(gate_n - 1):
        relay(k)
    loads[3].wait()
    loads[4].wait()
    for copy in near_gate:
        copy.wait_recv()

    def wait_go(i, _):
        go(me, partner(i)).wait_recv()
        return 0

    lax.fori_loop(0, ep_n - 1, wait_go, 0)

    def gated_slot(slot, _):
        rows = arrived[...].reshape(slots, width)
        activate(slot, dot(rows, gate_all[slot]), dot(rows, up_all[slot]))
        return 0

    lax.fori_loop(0, 2, gated_slot, 0)
    for k in range(gate_n - 1):
        for copy in relay_gate(k):
            copy.wait_recv()
    most = (gate_n - 1) * deep

    def most_slot(slot, _):
        rows = arrived[:, :, :most].reshape(slots, most)
        gate_sum[slot - 2] = dot(rows, gate_all[slot, :most])
        up_sum[slot - 2] = dot(rows, up_all[slot, :most])
        return 0

    lax.fori_loop(2, 4, most_slot, 0)
    relay(gate_n - 1)

    def last_slot(slot, _):
        @pl.when(slot == 3)
        def _():
            for copy in relay_gate(gate_n - 1):
                copy.wait_recv()

        rows = arrived[:, :, most:].reshape(slots, deep)
        activate(
            slot,
            gate_sum[slot - 2] + dot(rows, gate_all[slot, most:]),
            up_sum[slot - 2] + dot(rows, up_all[slot, most:]),
        )
        return 0

    lax.fori_loop(2, 4, last_slot, 0)

    def peer_of(i):
        return (mine + 1 + i) % half

    def back(c, peer, slot):
        return pltpu.make_async_remote_copy(
            src_ref=result.at[c, first + peer],
            dst_ref=returned.at[c, slot],
            send_sem=back_s.at[c, first + peer],
            recv_sem=back_r.at[c, slot],
            device_id=(first + peer, own),
            device_id_type=MESH,
        )

    def group(c, i, slot):
        return pltpu.make_async_remote_copy(
            src_ref=result.at[c, other + i],
            dst_ref=relay_in.at[c, i // plane, slot],
            send_sem=back_s.at[c, other + i],
            recv_sem=group_r.at[c, i // plane, slot],
            device_id=(relays + i % plane, own),
            device_id_type=MESH,
        )

    def dense_to(c, k):
        return pltpu.make_async_remote_copy(
            src_ref=relay_out.at[c, k],
            dst_ref=dense.at[c],
            send_sem=dense_s.at[c, k],
            recv_sem=dense_r.at[c],
            device_id=(other + k * plane + me % plane, own),
            device_id_type=MESH,
        )

    def weighed(at, values):
        return dot(merge_high[at], values) + dot(merge_low[at], values)

    def pass_on(c):
        for k in range(2):

            def wait_group(i, _):
                group(c, k * plane + me % plane, peer_of(i)).wait_recv()
                return 0

            lax.fori_loop(0, half - 1, wait_group, 0)
            values = relay_in[c, k].reshape(half * cap, part)
            relay_out[c, k] = weighed(1 + k, values).astype(BF16)
            dense_to(c, k).start()

    def down_part(c, _):
        far_down(c).wait_recv()
        relay_down(c).start()
        own_down(c).wait()
        near_down(c).wait_recv()
        relay_down(c).wait_recv()
        value = dot(hidden[...], down_all[c]).astype(BF16).reshape(ep_n, cap, part)
        result[c] = value

        def start_group(i, _):
            @pl.when(relays + i % plane != me)
            def _():
                group(c, i, mine).start()

            return 0

        lax.fori_loop(0, half, start_group, 0)

        def start_back(i, _):
            back(c, peer_of(i), mine).start()
            return 0

        lax.fori_loop(0, half - 1, start_back, 0)
        returned[c, mine] = result[c, me]

        @pl.when(is_relay)
        def _():
            for k in range(2):
                relay_in[c, k, mine] = result[c, other + k * plane + me % plane]

            @pl.when(c >= lag)
            def _():
                pass_on(c - lag)

        return 0

    lax.fori_loop(0, down_n, down_part, 0)

    @pl.when(is_relay)
    def _():
        def pass_rest(c, _):
            pass_on(c)
            return 0

        lax.fori_loop(down_n - lag, down_n, pass_rest, 0)

    def combine(c, _):
        def wait_back(i, _):
            back(c, mine, peer_of(i)).wait_recv()
            return 0

        lax.fori_loop(0, half - 1, wait_back, 0)
        pltpu.make_async_remote_copy(
            src_ref=dense.at[c],
            dst_ref=dense.at[c],
            send_sem=dense_s.at[c, 0],
            recv_sem=dense_r.at[c],
            device_id=(my_relay, own),
            device_id_type=MESH,
        ).wait_recv()
        values = returned[c].reshape(half * cap, part)
        expert_v[:, down_cols(c)] = (weighed(0, values) + dense[c].astype(F32)).astype(BF16)
        return 0

    lax.fori_loop(0, down_n, combine, 0)

    halo.wait_send()
    to_relay(routes_ref, near_routes.at[my_turn], 0).wait_send()
    to_relay(weight_ref, near_weights.at[my_turn], 1).wait_send()
    for k in range(gate_n):
        for copy in far_gate(k) + relay_gate(k):
            copy.wait_send()
    for copy in near_gate:
        copy.wait_send()

    def end_down(c, _):
        far_down(c).wait_send()
        relay_down(c).wait_send()
        near_down(c).wait_send()

        def end_back(i, _):
            back(c, peer_of(i), mine).wait_send()
            return 0

        lax.fori_loop(0, half - 1, end_back, 0)

        def end_group(i, _):
            @pl.when(relays + i % plane != me)
            def _():
                group(c, i, mine).wait_send()

            return 0

        lax.fori_loop(0, half, end_group, 0)

        @pl.when(is_relay)
        def _():
            for k in range(2):
                dense_to(c, k).wait_send()

        return 0

    lax.fori_loop(0, down_n, end_down, 0)

    def end_go(i, _):
        go(partner(i), me).wait_send()
        return 0

    lax.fori_loop(0, ep_n - 1, end_go, 0)


def on_device(
    pool_in,
    w_pool,
    pool_scale,
    w_out,
    expert_in,
    ffn_gain,
    routes,
    route_weight,
    w_gate,
    w_up,
    w_down,
):
    ep_n = lax.axis_size("ep")
    tp_n = lax.axis_size("tp")
    assert tp_n == 4 and ep_n % 4 == 0 and w_gate.shape[0] == 1
    half = ep_n // 2
    block_rows = routes.shape[0] // tp_n
    capacity = 3 * block_rows * K // (2 * ep_n)
    cap = -(-capacity // 16) * 16
    width = expert_in.shape[1]
    rows_here, pool_width = pool_in.shape
    local = w_gate.shape[2]
    slots = ep_n * cap
    down_n = 8
    part = width // down_n
    gate_n = 8
    vmem = pl.BlockSpec(memory_space=pltpu.VMEM)
    hbm = pl.BlockSpec(memory_space=pl.ANY)
    dma = pltpu.SemaphoreType.DMA
    return pl.pallas_call(
        functools.partial(kernel, (ep_n, tp_n, cap, gate_n, down_n)),
        out_shape=(
            pltpu.VMEM((rows_here, width), BF16),
            pltpu.VMEM((block_rows, width), BF16),
        ),
        in_specs=[vmem] * 4 + [hbm] * 7,
        out_specs=(vmem, vmem),
        scratch_shapes=[
            pltpu.VMEM(w_pool.shape, BF16),
            pltpu.VMEM((rows_here, pool_width), BF16),
            pltpu.VMEM((WMAX, pool_width), BF16),
            pltpu.VMEM((pool_width, width), BF16),
            pltpu.VMEM((rows_here, pool_width), BF16),
            pltpu.VMEM((block_rows, width), BF16),
            pltpu.VMEM((block_rows, width), BF16),
            pltpu.VMEM((ep_n, cap, width), BF16),
            pltpu.VMEM((ep_n, cap, width), BF16),
            pltpu.VMEM((tp_n, width, local), BF16),
            pltpu.VMEM((tp_n, width, local), BF16),
            pltpu.VMEM((2, slots, local), F32),
            pltpu.VMEM((2, slots, local), F32),
            pltpu.VMEM((slots, tp_n * local), BF16),
            pltpu.VMEM((down_n, tp_n * local, part), BF16),
            pltpu.VMEM((down_n, ep_n, cap, part), BF16),
            pltpu.VMEM((down_n, half, cap, part), BF16),
            pltpu.VMEM((down_n, 2, half, cap, part), BF16),
            pltpu.VMEM((down_n, 2, block_rows, part), BF16),
            pltpu.VMEM((down_n, block_rows, part), BF16),
            pltpu.VMEM((2, K, block_rows), jnp.int32),
            pltpu.VMEM((2, K, block_rows), F32),
            pltpu.VMEM((3, block_rows, half * cap), BF16),
            pltpu.VMEM((3, block_rows, half * cap), BF16),
            dma((7 + down_n,)),
            dma((2 * gate_n + down_n,)),
            dma((2 * gate_n + down_n,)),
            dma((2 + down_n,)),
            dma((2 + down_n,)),
            dma((2 * gate_n + down_n,)),
            dma((2 * gate_n + down_n,)),
            dma((ep_n,)),
            dma((ep_n,)),
            dma((down_n, ep_n)),
            dma((down_n, half)),
            dma((down_n, 2, half)),
            dma((down_n, 2)),
            dma((down_n,)),
            dma((2,)),
            dma((2, 2)),
            dma,
            dma,
            pltpu.SemaphoreType.REGULAR,
            pltpu.SemaphoreType.REGULAR,
        ],
        compiler_params=pltpu.CompilerParams(
            collective_id=0, has_side_effects=True, vmem_limit_bytes=60 * 1024 * 1024
        ),
    )(
        routes.T,
        route_weight.T,
        ffn_gain.reshape(1, -1),
        pool_scale.reshape(1, -1),
        w_pool,
        pool_in,
        w_out,
        expert_in,
        w_gate,
        w_up,
        w_down,
    )


def solution(mesh):
    placed = (
        P(("ep", "tp"), None),
        P(),
        P(),
        P(),
        P("ep", None),
        P(),
        P("ep", None),
        P("ep", None),
        P("ep", None, "tp"),
        P("ep", None, "tp"),
        P("ep", "tp", None),
    )
    return jax.shard_map(
        on_device,
        mesh=mesh,
        in_specs=placed,
        out_specs=(P(("ep", "tp"), None), P(("ep", "tp"), None)),
        check_vma=False,
    )
```

```python
import functools

import jax
import jax.numpy as jnp
from jax import lax
from jax.experimental import pallas as pl
from jax.experimental.pallas import tpu as pltpu
from jax.sharding import PartitionSpec as P

GDIM = 128
WMAX = 16
K = 2
EPS = 0.05
MESH = pl.DeviceIdType.MESH
F32 = jnp.float32
BF16 = jnp.bfloat16
LANES = 128


def dot(a, b):
    return jnp.dot(a, b, preferred_element_type=F32)


def kernel(
    dims,
    routes_ref,
    weight_ref,
    gain_ref,
    scale_ref,
    wpool_hbm,
    pool_hbm,
    wout_hbm,
    rows_hbm,
    gate_hbm,
    up_hbm,
    down_hbm,
    mixer_v,
    expert_v,
    wpool_ref,
    pool_v,
    halo_v,
    wout_v,
    scaled_v,
    mine_v,
    normed_v,
    outgoing,
    arrived,
    gate_all,
    up_all,
    gate_sum,
    up_sum,
    hidden,
    down_all,
    result,
    returned,
    relay_in,
    relay_out,
    dense,
    near_routes,
    near_weights,
    merge_high,
    merge_low,
    local_sem,
    far_s,
    far_r,
    near_s,
    near_r,
    relay_s,
    relay_r,
    go_s,
    go_r,
    back_s,
    back_r,
    group_r,
    dense_s,
    dense_r,
    names_s,
    names_r,
    halo_s,
    halo_r,
    hello,
    ready,
):
    ep_n, tp_n, cap, gate_n, sizes = dims
    down_n = len(sizes)
    starts = [sum(sizes[:c]) for c in range(down_n)]
    me = lax.axis_index("ep")
    own = lax.axis_index("tp")
    near = own + 1 - 2 * (own % 2)
    far = (own + tp_n // 2) % tp_n
    index = me * tp_n + own
    total = ep_n * tp_n
    after = (index + 1) % total
    before = (index + total - 1) % total
    block_rows, width = mine_v.shape
    slots = ep_n * cap
    local = gate_hbm.shape[2]
    deep = width // gate_n

    half = ep_n // 2
    plane = ep_n // 4
    upper = me // half
    first = upper * half
    other = half - first
    mine = me - first
    relays = half - plane + upper * plane
    is_relay = (me >= half - plane) & (me < half + plane)
    my_relay = half - upper * plane + me % plane
    my_turn = mine // plane

    def partner(i):
        return (me + ep_n // 2 + ((i + 1) // 2) * (1 - 2 * (i % 2))) % ep_n

    barrier = pltpu.get_barrier_semaphore()

    lead = own < tp_n // 2
    follow = own >= tp_n // 2

    @pl.when(lead)
    def _():
        pl.semaphore_signal(barrier, inc=1, device_id=(me, far), device_id_type=MESH)

    def down_cols(c):
        return pl.ds(starts[c], sizes[c])

    loads = [
        pltpu.make_async_copy(
            rows_hbm.at[pl.ds(own * block_rows, block_rows)], mine_v, local_sem.at[0]
        ),
        pltpu.make_async_copy(pool_hbm, pool_v, local_sem.at[1]),
        pltpu.make_async_copy(wout_hbm, wout_v, local_sem.at[2]),
        pltpu.make_async_copy(gate_hbm.at[0], gate_all.at[0], local_sem.at[3]),
        pltpu.make_async_copy(up_hbm.at[0], up_all.at[0], local_sem.at[4]),
        pltpu.make_async_copy(wpool_hbm, wpool_ref, local_sem.at[5]),
    ]
    for i in (3, 4, 0, 1, 5):
        loads[i].start()

    def own_down(c):
        return pltpu.make_async_copy(
            down_hbm.at[0, :, down_cols(c)], down_all.at[0:local, down_cols(c)], local_sem.at[7 + c]
        )

    for c in range(down_n):
        own_down(c).start()
    loads[2].start()

    @pl.when(follow)
    def _():
        pl.semaphore_wait(barrier, 1)
        pl.semaphore_signal(hello, inc=1, device_id=(me, far), device_id_type=MESH)

    @pl.when(lead)
    def _():
        pl.semaphore_wait(hello, 1)

    def to_far(src, dst, at):
        return pltpu.make_async_remote_copy(
            src_ref=src,
            dst_ref=dst,
            send_sem=far_s.at[at],
            recv_sem=far_r.at[at],
            device_id=(me, far),
            device_id_type=MESH,
        )

    def to_near(src, dst, at, send, recv):
        return pltpu.make_async_remote_copy(
            src_ref=src,
            dst_ref=dst,
            send_sem=send.at[at],
            recv_sem=recv.at[at],
            device_id=(me, near),
            device_id_type=MESH,
        )

    def far_gate(k):
        some = pl.ds(k * deep, deep)
        return (
            to_far(gate_hbm.at[0, some], gate_all.at[2, some], 2 * k),
            to_far(up_hbm.at[0, some], up_all.at[2, some], 2 * k + 1),
        )

    def relay_gate(k):
        some = pl.ds(k * deep, deep)
        return (
            to_near(gate_all.at[2, some], gate_all.at[3, some], 2 * k, relay_s, relay_r),
            to_near(up_all.at[2, some], up_all.at[3, some], 2 * k + 1, relay_s, relay_r),
        )

    def far_down(c):
        return to_far(
            down_hbm.at[0, :, down_cols(c)],
            down_all.at[2 * local : 3 * local, down_cols(c)],
            2 * gate_n + c,
        )

    def relay_down(c):
        return to_near(
            down_all.at[2 * local : 3 * local, down_cols(c)],
            down_all.at[3 * local : 4 * local, down_cols(c)],
            2 * gate_n + c,
            relay_s,
            relay_r,
        )

    def near_down(c):
        return to_near(
            down_all.at[0:local, down_cols(c)],
            down_all.at[local : 2 * local, down_cols(c)],
            2 + c,
            near_s,
            near_r,
        )

    near_gate = (
        to_near(gate_all.at[0], gate_all.at[1], 0, near_s, near_r),
        to_near(up_all.at[0], up_all.at[1], 1, near_s, near_r),
    )
    rows_here = pool_v.shape[0]
    halo = pltpu.make_async_remote_copy(
        src_ref=pool_hbm.at[rows_here - WMAX :],
        dst_ref=halo_v,
        send_sem=halo_s,
        recv_sem=halo_r,
        device_id=(after // tp_n, after % tp_n),
        device_id_type=MESH,
    )

    def to_relay(src, dst, at):
        return pltpu.make_async_remote_copy(
            src_ref=src.at[:, pl.ds(pl.multiple_of(own * block_rows, block_rows), block_rows)],
            dst_ref=dst,
            send_sem=names_s.at[at],
            recv_sem=names_r.at[at, my_turn],
            device_id=(my_relay, own),
            device_id_type=MESH,
        )

    ahead = [copy for k in range(gate_n) for copy in far_gate(k)]
    for copy in ahead[:3]:
        copy.start()

    @pl.when(follow)
    def _():
        for copy in ahead[3:4]:
            copy.start()

    @pl.when(lead)
    def _():
        def greet(i, _):
            peer = (me + 1 + i) % ep_n
            pl.semaphore_signal(barrier, inc=1, device_id=(peer, own), device_id_type=MESH)
            return 0

        lax.fori_loop(0, ep_n - 1, greet, 0)
        beside = (me + ep_n - 1 + 2 * (own % 2)) % ep_n
        for there in ((me, near), (beside, near)):
            pl.semaphore_signal(barrier, inc=1, device_id=there, device_id_type=MESH)


    block = pl.ds(pl.multiple_of(own * block_rows, block_rows), block_rows)
    tall = max(ep_n, 16)
    expert_of = lax.broadcasted_iota(jnp.int32, (tall, block_rows), 0)
    earlier = (
        lax.broadcasted_iota(jnp.int32, (block_rows, block_rows), 0)
        < lax.broadcasted_iota(jnp.int32, (block_rows, block_rows), 1)
    )
    earlier = jnp.where(earlier, 1.0, 0.0).astype(BF16)

    def places(routes):
        names = [expert_of == routes[j : j + 1] for j in range(K)]
        named = jnp.where(names[0] | names[1], 1.0, 0.0).astype(BF16)
        rank = dot(named, earlier)
        return [
            routes[j : j + 1] * cap
            + jnp.sum(jnp.where(names[j], rank, 0.0), axis=0, keepdims=True).astype(jnp.int32)
            for j in range(K)
        ]

    def set_merge(at, place, weights):
        slot_of = first * cap + lax.broadcasted_iota(jnp.int32, (half * cap, block_rows), 0)
        merged = jnp.zeros((half * cap, block_rows), F32)
        for j in range(K):
            merged = merged + jnp.where(slot_of == place[j], weights[j : j + 1], 0.0)
        merge = merged.T
        high = merge.astype(BF16)
        merge_high[at] = high
        merge_low[at] = (merge - high.astype(F32)).astype(BF16)

    place = places(routes_ref[:, block])
    slot_of = lax.broadcasted_iota(jnp.int32, (slots, block_rows), 0)
    spread = jnp.zeros((slots, block_rows), F32)
    for j in range(K):
        spread = spread + jnp.where(slot_of == place[j], 1.0, 0.0)
    spread = spread.astype(BF16)

    @pl.when(lead)
    def _():
        pl.semaphore_wait(barrier, ep_n + 1)
        pl.semaphore_signal(ready, inc=1, device_id=(me, far), device_id_type=MESH)

    @pl.when(follow)
    def _():
        pl.semaphore_wait(ready, 1)

    halo.start()

    @pl.when(lead)
    def _():
        for copy in ahead[3:4]:
            copy.start()

    for copy in ahead[4:]:
        copy.start()

    def start_far_down(c, _):
        far_down(c).start()
        return 0

    for c in range(down_n):
        own_down(c).wait()
        start_far_down(c, 0)
    to_relay(routes_ref, near_routes.at[my_turn], 0).start()
    to_relay(weight_ref, near_weights.at[my_turn], 1).start()

    loads[0].wait()
    features = mine_v[...].astype(F32)
    inverse = lax.rsqrt(jnp.mean(features * features, axis=-1, keepdims=True) + EPS)
    normed_v[...] = (features * inverse * gain_ref[...]).astype(BF16)

    step = 512
    lag = 2
    late = 2

    def spread_cols(i, _):
        cols = pl.ds(pl.multiple_of(i * step, step), step)
        rows = dot(spread, normed_v[:, cols]).astype(BF16)
        outgoing[:, :, cols] = rows.reshape(ep_n, cap, step)
        return 0

    lax.fori_loop(0, width // step, spread_cols, 0)

    def go(peer, slot):
        return pltpu.make_async_remote_copy(
            src_ref=outgoing.at[peer],
            dst_ref=arrived.at[slot],
            send_sem=go_s.at[peer],
            recv_sem=go_r.at[slot],
            device_id=(peer, own),
            device_id_type=MESH,
        )

    def start_go(i, _):
        go(partner(i), me).start()
        return 0

    lax.fori_loop(0, ep_n - 1, start_go, 0)
    arrived[me] = outgoing[me]

    loads[3].wait()
    loads[4].wait()
    for copy in near_gate:
        copy.start()

    def start_near_down(c, _):
        near_down(c).start()
        return 0

    for c in range(down_n):
        start_near_down(c, 0)

    set_merge(0, place, weight_ref[:, block])

    loads[1].wait()
    loads[5].wait()
    halo.wait_recv()
    position = (
        index * rows_here + lax.broadcasted_iota(jnp.int32, (rows_here, GDIM), 0)
    ).astype(F32)
    for g in range(wpool_ref.shape[0]):
        window = 2 ** (1 + g % 4)
        cols = slice(g * GDIM, (g + 1) * GDIM)
        head = jnp.where(index > 0, halo_v[:, cols].astype(F32), 0.0)
        here = pool_v[:, cols].astype(F32)
        running = jnp.concatenate([head, here], axis=0)
        shift = 1
        while shift < window:
            running = running + pltpu.roll(running, shift, 0)
            shift *= 2
        counted = jnp.minimum(position + 1.0, float(window))
        pooled = (running[WMAX:] / counted - here).astype(BF16)
        scaled_v[:, cols] = (dot(pooled, wpool_ref[g]) * scale_ref[:, cols]).astype(BF16)
    loads[2].wait()

    def mix_cols(i, _):
        cols = pl.ds(pl.multiple_of(i * step, step), step)
        mixer_v[:, cols] = dot(scaled_v[...], wout_v[:, cols]).astype(BF16)
        return 0

    lax.fori_loop(0, width // step, mix_cols, 0)

    @pl.when(is_relay)
    def _():
        for k in range(2):
            for at, held in enumerate((near_routes, near_weights)):
                pltpu.make_async_remote_copy(
                    src_ref=held.at[k],
                    dst_ref=held.at[k],
                    send_sem=names_s.at[at],
                    recv_sem=names_r.at[at, k],
                    device_id=(my_relay, own),
                    device_id_type=MESH,
                ).wait_recv()
            set_merge(1 + k, places(near_routes[k]), near_weights[k])

    def activate(slot, gate_val, up_val):
        value = gate_val / (1.0 + jnp.exp(-gate_val)) * up_val
        cols = pl.ds(pl.multiple_of(slot * local, LANES), local)
        hidden[:, cols] = value.astype(BF16)

    def relay(k):
        for copy in far_gate(k):
            copy.wait_recv()
        for copy in relay_gate(k):
            copy.start()

    for k in range(gate_n - 1):
        relay(k)
    for copy in near_gate:
        copy.wait_recv()

    def wait_go(i, _):
        go(me, partner(i)).wait_recv()
        return 0

    lax.fori_loop(0, ep_n - 1, wait_go, 0)

    def gated_slot(slot, _):
        rows = arrived[...].reshape(slots, width)
        activate(slot, dot(rows, gate_all[slot]), dot(rows, up_all[slot]))
        return 0

    lax.fori_loop(0, 2, gated_slot, 0)
    for k in range(gate_n - 1):
        for copy in relay_gate(k):
            copy.wait_recv()
    most = (gate_n - 1) * deep

    def most_slot(slot, _):
        rows = arrived[:, :, :most].reshape(slots, most)
        gate_sum[slot - 2] = dot(rows, gate_all[slot, :most])
        up_sum[slot - 2] = dot(rows, up_all[slot, :most])
        return 0

    lax.fori_loop(2, 4, most_slot, 0)
    relay(gate_n - 1)

    def last_slot(slot, _):
        @pl.when(slot == 3)
        def _():
            for copy in relay_gate(gate_n - 1):
                copy.wait_recv()

        rows = arrived[:, :, most:].reshape(slots, deep)
        activate(
            slot,
            gate_sum[slot - 2] + dot(rows, gate_all[slot, most:]),
            up_sum[slot - 2] + dot(rows, up_all[slot, most:]),
        )
        return 0

    lax.fori_loop(2, 4, last_slot, 0)

    def peer_of(i):
        return (mine + 1 + i) % half

    def back(c, peer, slot):
        return pltpu.make_async_remote_copy(
            src_ref=result.at[first + peer, :, down_cols(c)],
            dst_ref=returned.at[slot, :, down_cols(c)],
            send_sem=back_s.at[c, first + peer],
            recv_sem=back_r.at[c, slot],
            device_id=(first + peer, own),
            device_id_type=MESH,
        )

    def group(c, i, slot):
        return pltpu.make_async_remote_copy(
            src_ref=result.at[other + i, :, down_cols(c)],
            dst_ref=relay_in.at[i // plane, slot, :, down_cols(c)],
            send_sem=back_s.at[c, other + i],
            recv_sem=group_r.at[c, i // plane, slot],
            device_id=(relays + i % plane, own),
            device_id_type=MESH,
        )

    def dense_to(c, k):
        return pltpu.make_async_remote_copy(
            src_ref=relay_out.at[k, :, down_cols(c)],
            dst_ref=dense.at[:, down_cols(c)],
            send_sem=dense_s.at[c, k],
            recv_sem=dense_r.at[c],
            device_id=(other + k * plane + me % plane, own),
            device_id_type=MESH,
        )

    def weighed(at, values):
        return dot(merge_high[at], values) + dot(merge_low[at], values)

    def pass_on(c):
        for k in range(2):

            def wait_group(i, _):
                group(c, k * plane + me % plane, peer_of(i)).wait_recv()
                return 0

            lax.fori_loop(0, half - 1, wait_group, 0)
            values = relay_in[k, :, :, down_cols(c)].reshape(half * cap, sizes[c])
            relay_out[k, :, down_cols(c)] = weighed(1 + k, values).astype(BF16)
            dense_to(c, k).start()

    def start_backs(c):
        def start_back(i, _):
            back(c, peer_of(i), mine).start()
            return 0

        lax.fori_loop(0, half - 1, start_back, 0)

    def down_part(c, _):
        far_down(c).wait_recv()
        relay_down(c).start()
        near_down(c).wait_recv()
        relay_down(c).wait_recv()
        value = dot(hidden[...], down_all[:, down_cols(c)]).astype(BF16)
        result[:, :, down_cols(c)] = value.reshape(ep_n, cap, sizes[c])

        def start_group(i, _):
            @pl.when(relays + i % plane != me)
            def _():
                group(c, i, mine).start()

            return 0

        lax.fori_loop(0, half, start_group, 0)

        if c >= late:
            start_backs(c - late)
        returned[mine, :, down_cols(c)] = result[me, :, down_cols(c)]

        @pl.when(is_relay)
        def _():
            for k in range(2):
                far_rows = result[other + k * plane + me % plane, :, down_cols(c)]
                relay_in[k, mine, :, down_cols(c)] = far_rows

            if c >= lag:
                pass_on(c - lag)

        return 0

    for c in range(down_n):
        down_part(c, 0)
    for c in range(down_n - late, down_n):
        start_backs(c)

    @pl.when(is_relay)
    def _():
        for c in range(down_n - lag, down_n):
            pass_on(c)

    def combine(c, _):
        def wait_back(i, _):
            back(c, mine, peer_of(i)).wait_recv()
            return 0

        lax.fori_loop(0, half - 1, wait_back, 0)
        pltpu.make_async_remote_copy(
            src_ref=dense.at[:, down_cols(c)],
            dst_ref=dense.at[:, down_cols(c)],
            send_sem=dense_s.at[c, 0],
            recv_sem=dense_r.at[c],
            device_id=(my_relay, own),
            device_id_type=MESH,
        ).wait_recv()
        values = returned[:, :, down_cols(c)].reshape(half * cap, sizes[c])
        total_val = weighed(0, values) + dense[:, down_cols(c)].astype(F32)
        expert_v[:, down_cols(c)] = total_val.astype(BF16)
        return 0

    for c in range(down_n):
        combine(c, 0)

    halo.wait_send()
    to_relay(routes_ref, near_routes.at[my_turn], 0).wait_send()
    to_relay(weight_ref, near_weights.at[my_turn], 1).wait_send()
    for k in range(gate_n):
        for copy in far_gate(k) + relay_gate(k):
            copy.wait_send()
    for copy in near_gate:
        copy.wait_send()

    def end_down(c, _):
        far_down(c).wait_send()
        relay_down(c).wait_send()
        near_down(c).wait_send()

        def end_back(i, _):
            back(c, peer_of(i), mine).wait_send()
            return 0

        lax.fori_loop(0, half - 1, end_back, 0)

        def end_group(i, _):
            @pl.when(relays + i % plane != me)
            def _():
                group(c, i, mine).wait_send()

            return 0

        lax.fori_loop(0, half, end_group, 0)

        @pl.when(is_relay)
        def _():
            for k in range(2):
                dense_to(c, k).wait_send()

        return 0

    for c in range(down_n):
        end_down(c, 0)

    def end_go(i, _):
        go(partner(i), me).wait_send()
        return 0

    lax.fori_loop(0, ep_n - 1, end_go, 0)


def on_device(
    pool_in,
    w_pool,
    pool_scale,
    w_out,
    expert_in,
    ffn_gain,
    routes,
    route_weight,
    w_gate,
    w_up,
    w_down,
):
    ep_n = lax.axis_size("ep")
    tp_n = lax.axis_size("tp")
    assert tp_n == 4 and ep_n % 4 == 0 and w_gate.shape[0] == 1
    half = ep_n // 2
    block_rows = routes.shape[0] // tp_n
    capacity = 3 * block_rows * K // (2 * ep_n)
    cap = -(-capacity // 16) * 16
    width = expert_in.shape[1]
    rows_here, pool_width = pool_in.shape
    local = w_gate.shape[2]
    slots = ep_n * cap
    sizes = (width // 8,) * 8
    down_n = len(sizes)
    gate_n = 8
    vmem = pl.BlockSpec(memory_space=pltpu.VMEM)
    hbm = pl.BlockSpec(memory_space=pl.ANY)
    dma = pltpu.SemaphoreType.DMA
    return pl.pallas_call(
        functools.partial(kernel, (ep_n, tp_n, cap, gate_n, sizes)),
        out_shape=(
            pltpu.VMEM((rows_here, width), BF16),
            pltpu.VMEM((block_rows, width), BF16),
        ),
        in_specs=[vmem] * 4 + [hbm] * 7,
        out_specs=(vmem, vmem),
        scratch_shapes=[
            pltpu.VMEM(w_pool.shape, BF16),
            pltpu.VMEM((rows_here, pool_width), BF16),
            pltpu.VMEM((WMAX, pool_width), BF16),
            pltpu.VMEM((pool_width, width), BF16),
            pltpu.VMEM((rows_here, pool_width), BF16),
            pltpu.VMEM((block_rows, width), BF16),
            pltpu.VMEM((block_rows, width), BF16),
            pltpu.VMEM((ep_n, cap, width), BF16),
            pltpu.VMEM((ep_n, cap, width), BF16),
            pltpu.VMEM((tp_n, width, local), BF16),
            pltpu.VMEM((tp_n, width, local), BF16),
            pltpu.VMEM((2, slots, local), F32),
            pltpu.VMEM((2, slots, local), F32),
            pltpu.VMEM((slots, tp_n * local), BF16),
            pltpu.VMEM((tp_n * local, width), BF16),
            pltpu.VMEM((ep_n, cap, width), BF16),
            pltpu.VMEM((half, cap, width), BF16),
            pltpu.VMEM((2, half, cap, width), BF16),
            pltpu.VMEM((2, block_rows, width), BF16),
            pltpu.VMEM((block_rows, width), BF16),
            pltpu.VMEM((2, K, block_rows), jnp.int32),
            pltpu.VMEM((2, K, block_rows), F32),
            pltpu.VMEM((3, block_rows, half * cap), BF16),
            pltpu.VMEM((3, block_rows, half * cap), BF16),
            dma((7 + down_n,)),
            dma((2 * gate_n + down_n,)),
            dma((2 * gate_n + down_n,)),
            dma((2 + down_n,)),
            dma((2 + down_n,)),
            dma((2 * gate_n + down_n,)),
            dma((2 * gate_n + down_n,)),
            dma((ep_n,)),
            dma((ep_n,)),
            dma((down_n, ep_n)),
            dma((down_n, half)),
            dma((down_n, 2, half)),
            dma((down_n, 2)),
            dma((down_n,)),
            dma((2,)),
            dma((2, 2)),
            dma,
            dma,
            pltpu.SemaphoreType.REGULAR,
            pltpu.SemaphoreType.REGULAR,
        ],
        compiler_params=pltpu.CompilerParams(
            collective_id=0, has_side_effects=True, vmem_limit_bytes=60 * 1024 * 1024
        ),
    )(
        routes.T,
        route_weight.T,
        ffn_gain.reshape(1, -1),
        pool_scale.reshape(1, -1),
        w_pool,
        pool_in,
        w_out,
        expert_in,
        w_gate,
        w_up,
        w_down,
    )


def solution(mesh):
    placed = (
        P(("ep", "tp"), None),
        P(),
        P(),
        P(),
        P("ep", None),
        P(),
        P("ep", None),
        P("ep", None),
        P("ep", None, "tp"),
        P("ep", None, "tp"),
        P("ep", "tp", None),
    )
    return jax.shard_map(
        on_device,
        mesh=mesh,
        in_specs=placed,
        out_specs=(P(("ep", "tp"), None), P(("ep", "tp"), None)),
        check_vma=False,
    )
```

```python
import functools

import jax
import jax.numpy as jnp
from jax import lax
from jax.experimental import pallas as pl
from jax.experimental.pallas import tpu as pltpu
from jax.sharding import PartitionSpec as P

GDIM = 128
WMAX = 16
K = 2
EPS = 0.05
MESH = pl.DeviceIdType.MESH
F32 = jnp.float32
BF16 = jnp.bfloat16
LANES = 128


def dot(a, b):
    return jnp.dot(a, b, preferred_element_type=F32)


def kernel(
    dims,
    routes_ref,
    weight_ref,
    gain_ref,
    scale_ref,
    wpool_hbm,
    pool_hbm,
    wout_hbm,
    rows_hbm,
    gate_hbm,
    up_hbm,
    down_hbm,
    mixer_v,
    expert_v,
    wpool_ref,
    pool_v,
    halo_v,
    wout_v,
    scaled_v,
    mine_v,
    normed_v,
    outgoing,
    arrived,
    gate_all,
    up_all,
    gate_sum,
    up_sum,
    hidden,
    down_all,
    result,
    returned,
    relay_in,
    relay_out,
    dense,
    near_routes,
    near_weights,
    merge_high,
    merge_low,
    local_sem,
    far_s,
    far_r,
    near_s,
    near_r,
    relay_s,
    relay_r,
    go_s,
    go_r,
    back_s,
    back_r,
    group_r,
    dense_s,
    dense_r,
    names_s,
    names_r,
    halo_s,
    halo_r,
    hello,
    ready,
):
    ep_n, tp_n, cap, gate_n, sizes = dims
    down_n = len(sizes)
    starts = [sum(sizes[:c]) for c in range(down_n)]
    me = lax.axis_index("ep")
    own = lax.axis_index("tp")
    near = own + 1 - 2 * (own % 2)
    far = (own + tp_n // 2) % tp_n
    index = me * tp_n + own
    total = ep_n * tp_n
    after = (index + 1) % total
    before = (index + total - 1) % total
    block_rows, width = mine_v.shape
    slots = ep_n * cap
    local = gate_hbm.shape[2]
    deep = width // gate_n

    half = ep_n // 2
    plane = ep_n // 4
    upper = me // half
    first = upper * half
    other = half - first
    mine = me - first
    relays = half - plane + upper * plane
    is_relay = (me >= half - plane) & (me < half + plane)
    my_relay = half - upper * plane + me % plane
    my_turn = mine // plane

    def partner(i):
        return (me + ep_n // 2 + ((i + 1) // 2) * (1 - 2 * (i % 2))) % ep_n

    barrier = pltpu.get_barrier_semaphore()

    lead = own < tp_n // 2
    follow = own >= tp_n // 2

    @pl.when(lead)
    def _():
        pl.semaphore_signal(barrier, inc=1, device_id=(me, far), device_id_type=MESH)

    def down_cols(c):
        return pl.ds(starts[c], sizes[c])

    loads = [
        pltpu.make_async_copy(
            rows_hbm.at[pl.ds(own * block_rows, block_rows)], mine_v, local_sem.at[0]
        ),
        pltpu.make_async_copy(pool_hbm, pool_v, local_sem.at[1]),
        pltpu.make_async_copy(wout_hbm, wout_v, local_sem.at[2]),
        pltpu.make_async_copy(gate_hbm.at[0], gate_all.at[0], local_sem.at[3]),
        pltpu.make_async_copy(up_hbm.at[0], up_all.at[0], local_sem.at[4]),
        pltpu.make_async_copy(wpool_hbm, wpool_ref, local_sem.at[5]),
    ]
    for i in (3, 4, 0, 1, 5):
        loads[i].start()

    def own_down(c):
        return pltpu.make_async_copy(
            down_hbm.at[0, :, down_cols(c)], down_all.at[0:local, down_cols(c)], local_sem.at[7 + c]
        )

    for c in range(down_n):
        own_down(c).start()
    loads[2].start()

    @pl.when(follow)
    def _():
        pl.semaphore_wait(barrier, 1)
        pl.semaphore_signal(hello, inc=1, device_id=(me, far), device_id_type=MESH)

    @pl.when(lead)
    def _():
        pl.semaphore_wait(hello, 1)

    def to_far(src, dst, at):
        return pltpu.make_async_remote_copy(
            src_ref=src,
            dst_ref=dst,
            send_sem=far_s.at[at],
            recv_sem=far_r.at[at],
            device_id=(me, far),
            device_id_type=MESH,
        )

    def to_near(src, dst, at, send, recv):
        return pltpu.make_async_remote_copy(
            src_ref=src,
            dst_ref=dst,
            send_sem=send.at[at],
            recv_sem=recv.at[at],
            device_id=(me, near),
            device_id_type=MESH,
        )

    def far_gate(k):
        some = pl.ds(k * deep, deep)
        return (
            to_far(gate_hbm.at[0, some], gate_all.at[2, some], 2 * k),
            to_far(up_hbm.at[0, some], up_all.at[2, some], 2 * k + 1),
        )

    def relay_gate(k):
        some = pl.ds(k * deep, deep)
        return (
            to_near(gate_all.at[2, some], gate_all.at[3, some], 2 * k, relay_s, relay_r),
            to_near(up_all.at[2, some], up_all.at[3, some], 2 * k + 1, relay_s, relay_r),
        )

    def far_down(c):
        return to_far(
            down_hbm.at[0, :, down_cols(c)],
            down_all.at[2 * local : 3 * local, down_cols(c)],
            2 * gate_n + c,
        )

    def relay_down(c):
        return to_near(
            down_all.at[2 * local : 3 * local, down_cols(c)],
            down_all.at[3 * local : 4 * local, down_cols(c)],
            2 * gate_n + c,
            relay_s,
            relay_r,
        )

    def near_down(c):
        return to_near(
            down_all.at[0:local, down_cols(c)],
            down_all.at[local : 2 * local, down_cols(c)],
            2 + c,
            near_s,
            near_r,
        )

    near_gate = (
        to_near(gate_all.at[0], gate_all.at[1], 0, near_s, near_r),
        to_near(up_all.at[0], up_all.at[1], 1, near_s, near_r),
    )
    rows_here = pool_v.shape[0]
    halo = pltpu.make_async_remote_copy(
        src_ref=pool_hbm.at[rows_here - WMAX :],
        dst_ref=halo_v,
        send_sem=halo_s,
        recv_sem=halo_r,
        device_id=(after // tp_n, after % tp_n),
        device_id_type=MESH,
    )

    def to_relay(src, dst, at):
        return pltpu.make_async_remote_copy(
            src_ref=src.at[:, pl.ds(pl.multiple_of(own * block_rows, block_rows), block_rows)],
            dst_ref=dst,
            send_sem=names_s.at[at],
            recv_sem=names_r.at[at, my_turn],
            device_id=(my_relay, own),
            device_id_type=MESH,
        )

    ahead = [copy for k in range(gate_n) for copy in far_gate(k)]
    for copy in ahead[:3]:
        copy.start()

    @pl.when(follow)
    def _():
        for copy in ahead[3:4]:
            copy.start()

    @pl.when(lead)
    def _():
        def greet(i, _):
            peer = (me + 1 + i) % ep_n
            pl.semaphore_signal(barrier, inc=1, device_id=(peer, own), device_id_type=MESH)
            return 0

        lax.fori_loop(0, ep_n - 1, greet, 0)
        beside = (me + ep_n - 1 + 2 * (own % 2)) % ep_n
        for there in ((me, near), (beside, near)):
            pl.semaphore_signal(barrier, inc=1, device_id=there, device_id_type=MESH)


    block = pl.ds(pl.multiple_of(own * block_rows, block_rows), block_rows)
    tall = max(ep_n, 16)
    expert_of = lax.broadcasted_iota(jnp.int32, (tall, block_rows), 0)
    earlier = (
        lax.broadcasted_iota(jnp.int32, (block_rows, block_rows), 0)
        < lax.broadcasted_iota(jnp.int32, (block_rows, block_rows), 1)
    )
    earlier = jnp.where(earlier, 1.0, 0.0).astype(BF16)

    def places(routes):
        names = [expert_of == routes[j : j + 1] for j in range(K)]
        named = jnp.where(names[0] | names[1], 1.0, 0.0).astype(BF16)
        rank = dot(named, earlier)
        return [
            routes[j : j + 1] * cap
            + jnp.sum(jnp.where(names[j], rank, 0.0), axis=0, keepdims=True).astype(jnp.int32)
            for j in range(K)
        ]

    def set_merge(at, place, weights):
        slot_of = first * cap + lax.broadcasted_iota(jnp.int32, (half * cap, block_rows), 0)
        merged = jnp.zeros((half * cap, block_rows), F32)
        for j in range(K):
            merged = merged + jnp.where(slot_of == place[j], weights[j : j + 1], 0.0)
        merge = merged.T
        high = merge.astype(BF16)
        merge_high[at] = high
        merge_low[at] = (merge - high.astype(F32)).astype(BF16)

    place = places(routes_ref[:, block])
    slot_of = lax.broadcasted_iota(jnp.int32, (slots, block_rows), 0)
    spread = jnp.zeros((slots, block_rows), F32)
    for j in range(K):
        spread = spread + jnp.where(slot_of == place[j], 1.0, 0.0)
    spread = spread.astype(BF16)

    @pl.when(lead)
    def _():
        pl.semaphore_wait(barrier, ep_n + 1)
        pl.semaphore_signal(ready, inc=1, device_id=(me, far), device_id_type=MESH)

    @pl.when(follow)
    def _():
        pl.semaphore_wait(ready, 1)

    halo.start()

    @pl.when(lead)
    def _():
        for copy in ahead[3:4]:
            copy.start()

    for copy in ahead[4:]:
        copy.start()

    def start_far_down(c, _):
        far_down(c).start()
        return 0

    for c in range(down_n):
        own_down(c).wait()
        start_far_down(c, 0)
    to_relay(routes_ref, near_routes.at[my_turn], 0).start()
    to_relay(weight_ref, near_weights.at[my_turn], 1).start()

    loads[0].wait()
    features = mine_v[...].astype(F32)
    inverse = lax.rsqrt(jnp.mean(features * features, axis=-1, keepdims=True) + EPS)
    normed_v[...] = (features * inverse * gain_ref[...]).astype(BF16)

    step = 512
    lag = 2
    late = 2

    def spread_cols(i, _):
        cols = pl.ds(pl.multiple_of(i * step, step), step)
        rows = dot(spread, normed_v[:, cols]).astype(BF16)
        outgoing[:, :, cols] = rows.reshape(ep_n, cap, step)
        return 0

    lax.fori_loop(0, width // step, spread_cols, 0)

    def go(peer, slot):
        return pltpu.make_async_remote_copy(
            src_ref=outgoing.at[peer],
            dst_ref=arrived.at[slot],
            send_sem=go_s.at[peer],
            recv_sem=go_r.at[slot],
            device_id=(peer, own),
            device_id_type=MESH,
        )

    def start_go(i, _):
        go(partner(i), me).start()
        return 0

    lax.fori_loop(0, ep_n - 1, start_go, 0)
    arrived[me] = outgoing[me]

    loads[3].wait()
    loads[4].wait()
    for copy in near_gate:
        copy.start()

    def start_near_down(c, _):
        near_down(c).start()
        return 0

    for c in range(down_n):
        start_near_down(c, 0)

    set_merge(0, place, weight_ref[:, block])

    loads[1].wait()
    loads[5].wait()
    halo.wait_recv()
    position = (
        index * rows_here + lax.broadcasted_iota(jnp.int32, (rows_here, GDIM), 0)
    ).astype(F32)
    for g in range(wpool_ref.shape[0]):
        window = 2 ** (1 + g % 4)
        cols = slice(g * GDIM, (g + 1) * GDIM)
        head = jnp.where(index > 0, halo_v[:, cols].astype(F32), 0.0)
        here = pool_v[:, cols].astype(F32)
        running = jnp.concatenate([head, here], axis=0)
        shift = 1
        while shift < window:
            running = running + pltpu.roll(running, shift, 0)
            shift *= 2
        counted = jnp.minimum(position + 1.0, float(window))
        pooled = (running[WMAX:] / counted - here).astype(BF16)
        scaled_v[:, cols] = (dot(pooled, wpool_ref[g]) * scale_ref[:, cols]).astype(BF16)
    loads[2].wait()

    def mix_cols(i, _):
        cols = pl.ds(pl.multiple_of(i * step, step), step)
        mixer_v[:, cols] = dot(scaled_v[...], wout_v[:, cols]).astype(BF16)
        return 0

    lax.fori_loop(0, width // step, mix_cols, 0)

    @pl.when(is_relay)
    def _():
        for k in range(2):
            for at, held in enumerate((near_routes, near_weights)):
                pltpu.make_async_remote_copy(
                    src_ref=held.at[k],
                    dst_ref=held.at[k],
                    send_sem=names_s.at[at],
                    recv_sem=names_r.at[at, k],
                    device_id=(my_relay, own),
                    device_id_type=MESH,
                ).wait_recv()
            set_merge(1 + k, places(near_routes[k]), near_weights[k])

    def activate(slot, gate_val, up_val):
        value = gate_val / (1.0 + jnp.exp(-gate_val)) * up_val
        cols = pl.ds(pl.multiple_of(slot * local, LANES), local)
        hidden[:, cols] = value.astype(BF16)

    def relay(k):
        for copy in far_gate(k):
            copy.wait_recv()
        for copy in relay_gate(k):
            copy.start()

    for k in range(gate_n - 1):
        relay(k)
    for copy in near_gate:
        copy.wait_recv()

    def wait_go(i, _):
        go(me, partner(i)).wait_recv()
        return 0

    lax.fori_loop(0, ep_n - 1, wait_go, 0)

    def gated_slot(slot, _):
        rows = arrived[...].reshape(slots, width)
        activate(slot, dot(rows, gate_all[slot]), dot(rows, up_all[slot]))
        return 0

    lax.fori_loop(0, 2, gated_slot, 0)
    for k in range(gate_n - 1):
        for copy in relay_gate(k):
            copy.wait_recv()
    most = (gate_n - 1) * deep

    def most_slot(slot, _):
        rows = arrived[:, :, :most].reshape(slots, most)
        gate_sum[slot - 2] = dot(rows, gate_all[slot, :most])
        up_sum[slot - 2] = dot(rows, up_all[slot, :most])
        return 0

    lax.fori_loop(2, 4, most_slot, 0)
    relay(gate_n - 1)

    def last_slot(slot, _):
        @pl.when(slot == 3)
        def _():
            for copy in relay_gate(gate_n - 1):
                copy.wait_recv()

        rows = arrived[:, :, most:].reshape(slots, deep)
        activate(
            slot,
            gate_sum[slot - 2] + dot(rows, gate_all[slot, most:]),
            up_sum[slot - 2] + dot(rows, up_all[slot, most:]),
        )
        return 0

    lax.fori_loop(2, 4, last_slot, 0)

    def peer_of(i):
        return (mine + 1 + i) % half

    def back(c, peer, slot):
        return pltpu.make_async_remote_copy(
            src_ref=result.at[first + peer, :, down_cols(c)],
            dst_ref=returned.at[slot, :, down_cols(c)],
            send_sem=back_s.at[c, first + peer],
            recv_sem=back_r.at[c, slot],
            device_id=(first + peer, own),
            device_id_type=MESH,
        )

    def group(c, i, slot):
        return pltpu.make_async_remote_copy(
            src_ref=result.at[other + i, :, down_cols(c)],
            dst_ref=relay_in.at[i // plane, slot, :, down_cols(c)],
            send_sem=back_s.at[c, other + i],
            recv_sem=group_r.at[c, i // plane, slot],
            device_id=(relays + i % plane, own),
            device_id_type=MESH,
        )

    def dense_to(c, k):
        return pltpu.make_async_remote_copy(
            src_ref=relay_out.at[k, :, down_cols(c)],
            dst_ref=dense.at[:, down_cols(c)],
            send_sem=dense_s.at[c, k],
            recv_sem=dense_r.at[c],
            device_id=(other + k * plane + me % plane, own),
            device_id_type=MESH,
        )

    def weighed(at, values):
        both = jnp.concatenate([merge_high[at], merge_low[at]], axis=0)
        value = dot(both, values)
        return value[:block_rows] + value[block_rows:]

    def pass_on(c):
        for k in range(2):

            def wait_group(i, _):
                group(c, k * plane + me % plane, peer_of(i)).wait_recv()
                return 0

            lax.fori_loop(0, half - 1, wait_group, 0)
            values = relay_in[k, :, :, down_cols(c)].reshape(half * cap, sizes[c])
            relay_out[k, :, down_cols(c)] = weighed(1 + k, values).astype(BF16)
            dense_to(c, k).start()

    def start_backs(c):
        def start_back(i, _):
            back(c, peer_of(i), mine).start()
            return 0

        lax.fori_loop(0, half - 1, start_back, 0)

    def down_part(c, _):
        far_down(c).wait_recv()
        relay_down(c).start()
        near_down(c).wait_recv()
        held = 3 * local
        value = dot(hidden[:, :held], down_all[:held, down_cols(c)])
        relay_down(c).wait_recv()
        value = value + dot(hidden[:, held:], down_all[held:, down_cols(c)])
        value = value.astype(BF16)
        result[:, :, down_cols(c)] = value.reshape(ep_n, cap, sizes[c])

        def start_group(i, _):
            @pl.when(relays + i % plane != me)
            def _():
                group(c, i, mine).start()

            return 0

        lax.fori_loop(0, half, start_group, 0)

        if c >= late:
            start_backs(c - late)
        returned[mine, :, down_cols(c)] = result[me, :, down_cols(c)]

        @pl.when(is_relay)
        def _():
            for k in range(2):
                far_rows = result[other + k * plane + me % plane, :, down_cols(c)]
                relay_in[k, mine, :, down_cols(c)] = far_rows

            if c >= lag:
                pass_on(c - lag)

        return 0

    for c in range(down_n):
        down_part(c, 0)
    for c in range(down_n - late, down_n):
        start_backs(c)

    @pl.when(is_relay)
    def _():
        for c in range(down_n - lag, down_n):
            pass_on(c)

    def combine(c, _):
        def wait_back(i, _):
            back(c, mine, peer_of(i)).wait_recv()
            return 0

        lax.fori_loop(0, half - 1, wait_back, 0)
        pltpu.make_async_remote_copy(
            src_ref=dense.at[:, down_cols(c)],
            dst_ref=dense.at[:, down_cols(c)],
            send_sem=dense_s.at[c, 0],
            recv_sem=dense_r.at[c],
            device_id=(my_relay, own),
            device_id_type=MESH,
        ).wait_recv()
        values = returned[:, :, down_cols(c)].reshape(half * cap, sizes[c])
        total_val = weighed(0, values) + dense[:, down_cols(c)].astype(F32)
        expert_v[:, down_cols(c)] = total_val.astype(BF16)
        return 0

    for c in range(down_n):
        combine(c, 0)

    halo.wait_send()
    to_relay(routes_ref, near_routes.at[my_turn], 0).wait_send()
    to_relay(weight_ref, near_weights.at[my_turn], 1).wait_send()
    for k in range(gate_n):
        for copy in far_gate(k) + relay_gate(k):
            copy.wait_send()
    for copy in near_gate:
        copy.wait_send()

    def end_down(c, _):
        far_down(c).wait_send()
        relay_down(c).wait_send()
        near_down(c).wait_send()

        def end_back(i, _):
            back(c, peer_of(i), mine).wait_send()
            return 0

        lax.fori_loop(0, half - 1, end_back, 0)

        def end_group(i, _):
            @pl.when(relays + i % plane != me)
            def _():
                group(c, i, mine).wait_send()

            return 0

        lax.fori_loop(0, half, end_group, 0)

        @pl.when(is_relay)
        def _():
            for k in range(2):
                dense_to(c, k).wait_send()

        return 0

    for c in range(down_n):
        end_down(c, 0)

    def end_go(i, _):
        go(partner(i), me).wait_send()
        return 0

    lax.fori_loop(0, ep_n - 1, end_go, 0)


def on_device(
    pool_in,
    w_pool,
    pool_scale,
    w_out,
    expert_in,
    ffn_gain,
    routes,
    route_weight,
    w_gate,
    w_up,
    w_down,
):
    ep_n = lax.axis_size("ep")
    tp_n = lax.axis_size("tp")
    assert tp_n == 4 and ep_n % 4 == 0 and w_gate.shape[0] == 1
    half = ep_n // 2
    block_rows = routes.shape[0] // tp_n
    capacity = 3 * block_rows * K // (2 * ep_n)
    cap = -(-capacity // 16) * 16
    width = expert_in.shape[1]
    rows_here, pool_width = pool_in.shape
    local = w_gate.shape[2]
    slots = ep_n * cap
    sizes = (width // 8,) * 8
    down_n = len(sizes)
    gate_n = 8
    vmem = pl.BlockSpec(memory_space=pltpu.VMEM)
    hbm = pl.BlockSpec(memory_space=pl.ANY)
    dma = pltpu.SemaphoreType.DMA
    return pl.pallas_call(
        functools.partial(kernel, (ep_n, tp_n, cap, gate_n, sizes)),
        out_shape=(
            pltpu.VMEM((rows_here, width), BF16),
            pltpu.VMEM((block_rows, width), BF16),
        ),
        in_specs=[vmem] * 4 + [hbm] * 7,
        out_specs=(vmem, vmem),
        scratch_shapes=[
            pltpu.VMEM(w_pool.shape, BF16),
            pltpu.VMEM((rows_here, pool_width), BF16),
            pltpu.VMEM((WMAX, pool_width), BF16),
            pltpu.VMEM((pool_width, width), BF16),
            pltpu.VMEM((rows_here, pool_width), BF16),
            pltpu.VMEM((block_rows, width), BF16),
            pltpu.VMEM((block_rows, width), BF16),
            pltpu.VMEM((ep_n, cap, width), BF16),
            pltpu.VMEM((ep_n, cap, width), BF16),
            pltpu.VMEM((tp_n, width, local), BF16),
            pltpu.VMEM((tp_n, width, local), BF16),
            pltpu.VMEM((2, slots, local), F32),
            pltpu.VMEM((2, slots, local), F32),
            pltpu.VMEM((slots, tp_n * local), BF16),
            pltpu.VMEM((tp_n * local, width), BF16),
            pltpu.VMEM((ep_n, cap, width), BF16),
            pltpu.VMEM((half, cap, width), BF16),
            pltpu.VMEM((2, half, cap, width), BF16),
            pltpu.VMEM((2, block_rows, width), BF16),
            pltpu.VMEM((block_rows, width), BF16),
            pltpu.VMEM((2, K, block_rows), jnp.int32),
            pltpu.VMEM((2, K, block_rows), F32),
            pltpu.VMEM((3, block_rows, half * cap), BF16),
            pltpu.VMEM((3, block_rows, half * cap), BF16),
            dma((7 + down_n,)),
            dma((2 * gate_n + down_n,)),
            dma((2 * gate_n + down_n,)),
            dma((2 + down_n,)),
            dma((2 + down_n,)),
            dma((2 * gate_n + down_n,)),
            dma((2 * gate_n + down_n,)),
            dma((ep_n,)),
            dma((ep_n,)),
            dma((down_n, ep_n)),
            dma((down_n, half)),
            dma((down_n, 2, half)),
            dma((down_n, 2)),
            dma((down_n,)),
            dma((2,)),
            dma((2, 2)),
            dma,
            dma,
            pltpu.SemaphoreType.REGULAR,
            pltpu.SemaphoreType.REGULAR,
        ],
        compiler_params=pltpu.CompilerParams(
            collective_id=0, has_side_effects=True, vmem_limit_bytes=60 * 1024 * 1024
        ),
    )(
        routes.T,
        route_weight.T,
        ffn_gain.reshape(1, -1),
        pool_scale.reshape(1, -1),
        w_pool,
        pool_in,
        w_out,
        expert_in,
        w_gate,
        w_up,
        w_down,
    )


def solution(mesh):
    placed = (
        P(("ep", "tp"), None),
        P(),
        P(),
        P(),
        P("ep", None),
        P(),
        P("ep", None),
        P("ep", None),
        P("ep", None, "tp"),
        P("ep", None, "tp"),
        P("ep", "tp", None),
    )
    return jax.shard_map(
        on_device,
        mesh=mesh,
        in_specs=placed,
        out_specs=(P(("ep", "tp"), None), P(("ep", "tp"), None)),
        check_vma=False,
    )
```
